512 devices in a mesh: rep: 2 (over z_hi), fs: 32 (over z_lo, y), tp: 8 (over x, core).
Axes of the slice: x: 4, y: 4, z: 16 (z_hi: 2, z_lo: 8; z = z_hi * 8 + z_lo), core: 2. Of those that a mesh axis runs over, the one named last changes fastest.
Arguments:
- inputs_next: bfloat16 [8192, 2048], P(('rep', 'fs'), 'tp'), parts along dimension 0, may hold values from -6 to 6
- inputs_prev: bfloat16 [8192, 2048], P(('rep', 'fs'), 'tp'), parts along dimension 0, may hold values from -6 to 6
- hidden_prev: bfloat16 [8192, 8192], P(('rep', 'fs')), parts along dimension 0, may hold values from -6 to 6
- cotangent: bfloat16 [8192, 2048], P(('rep', 'fs'), 'tp'), parts along dimension 0, may hold values from -6 to 6
- up_weight: bfloat16 [2048, 8192], P('tp', 'fs'), may hold values from -0.125 to 0.125
- down_weight: bfloat16 [8192, 2048], P('fs', 'tp'), may hold values from -0.0625 to 0.0625
- up_accum: float32 [4096, 8192], P(('rep', 'tp'), 'fs'), parts along dimension 0, may hold values from -192 to 192
- down_accum: float32 [16384, 2048], P(('rep', 'fs'), 'tp'), parts along dimension 0, may hold values from -192 to 192
Outputs:
- output_next: bfloat16 [8192, 2048], P(('rep', 'fs'), 'tp'), parts along dimension 0
- hidden_next: bfloat16 [8192, 8192], P(('rep', 'fs')), parts along dimension 0
- input_grad: bfloat16 [8192, 2048], P(('rep', 'fs'), 'tp'), parts along dimension 0
- up_accum_out: float32 [4096, 8192], P(('rep', 'tp'), 'fs'), parts along dimension 0
- down_accum_out: float32 [16384, 2048], P(('rep', 'fs'), 'tp'), parts along dimension 0
The draws below stay inside these ranges and needn't reach their ends.
There are 2 independent parts, one for each index of `rep`. The reference program is written for one: setup_inputs(seed, part) draws one part's arguments, and reference() takes and returns one part's arrays. A program takes and returns all parts, laid end to end along the dimension named above; an argument that names none is the same for every part. Nothing has to cross between parts.
All inputs are finite; a program needn't handle non-finite values.
Results may differ from the reference program's by a relative error of at most 0.034.
Values may be sent and summed in bfloat16 or wider, within the bound.
A program may use at most 128 MiB of HBM per device.

```python
import jax
import jax.numpy as jnp

D = 2048
FF = 8192
TOKENS = 4096
N_TP = 8


def with_spikes(drawn, rng, source, target, blocks, factor):
    owner, partner = [(jnp.arange(drawn.shape[axis_at]) // (drawn.shape[axis_at] // blocks)).reshape([-1 if axis == axis_at else 1 for axis in range(drawn.ndim)]) for axis_at in (source, target)]
    chosen = jax.random.permutation(rng, blocks)[partner]
    strong = (owner == chosen) | (owner == (partner + blocks // 2) % blocks)
    return jnp.where(strong, factor * drawn, drawn)


def level_of(rng, dims, shards, low, largest):
    loudness = 1.0
    for position, shards_of in shards:
        heights = jax.random.uniform(jax.random.fold_in(jax.random.fold_in(rng, 6), position), (shards_of,), jnp.float32, low / len(shards), largest / len(shards))
        loudness = loudness * jnp.repeat(jnp.exp(heights), dims[position] // shards_of).reshape((-1,) + (1,) * (len(dims) - 1 - position))
    return loudness


def centred(own_key, dims, scale, most, split=(), held_as=jnp.bfloat16):
    level = level_of(own_key, dims, split, -0.22, 0.18) if split else 1.0
    values = jax.random.normal(own_key, dims, jnp.float32) * scale * level
    return jnp.minimum(jnp.maximum(values, -most), most).astype(held_as)


def heavy_noise(key, shape, deviation, reach, pieces, heavy, kind=jnp.bfloat16):
    drawn = deviation * jax.random.normal(key, shape, jnp.float32)
    if pieces:
        drawn = drawn * level_of(key, shape, pieces, -0.22, 0.18)
    return jnp.clip(with_spikes(drawn, jax.random.fold_in(key, 3), *heavy), -reach, reach).astype(kind)


def setup_inputs(seed: int = 0, part: int = 0) -> dict:
    splits = jax.random.split(jax.random.key(seed), 9)
    part_splits = jax.random.split(jax.random.fold_in(splits[8], part), 9)
    inputs_next = centred(part_splits[0], (TOKENS, D), 1.0, 6.0, ((0, 32), (1, 8)))
    inputs_prev = centred(part_splits[1], (TOKENS, D), 1.0, 6.0, ((0, 32), (1, 8)))
    hidden_prev = centred(part_splits[2], (TOKENS, FF), 1.0, 6.0, ((0, 32),))
    cotangent = heavy_noise(part_splits[3], (TOKENS, D), 1.0, 6.0, ((0, 32), (1, 8)), (0, 1, 32, 2.75))
    up_weight = centred(splits[4], (D, FF), D ** -0.5, 0.125, ((0, 8), (1, 32)))
    down_weight = centred(splits[5], (FF, D), FF ** -0.5, 0.0625, ((0, 32), (1, 8)))
    up_accum = centred(part_splits[6], (D, FF), 32.0, 192.0, ((0, 8), (1, 32)), jnp.float32)
    down_accum = centred(part_splits[7], (FF, D), 32.0, 192.0, ((0, 32), (1, 8)), jnp.float32)
    return {"inputs_next": inputs_next, "inputs_prev": inputs_prev, "hidden_prev": hidden_prev, "cotangent": cotangent, "up_weight": up_weight, "down_weight": down_weight, "up_accum": up_accum, "down_accum": down_accum}


def squared_relu(values):
    return jnp.square(jax.nn.relu(values.astype(jnp.float32))).astype(jnp.bfloat16)


def reference(inputs_next, inputs_prev, hidden_prev, cotangent, up_weight, down_weight, up_accum, down_accum):
    col_width = D // N_TP
    row_total = inputs_next.shape[0]
    hidden_total = jnp.zeros((row_total, FF), jnp.float32)
    back_total = jnp.zeros((row_total, FF), jnp.float32)
    for block_index in range(N_TP):
        start_col = block_index * col_width
        partial_value = jnp.dot(inputs_next[:, start_col:start_col + col_width], up_weight[start_col:start_col + col_width, :], preferred_element_type=jnp.float32)
        hidden_total = hidden_total + partial_value.astype(jnp.bfloat16).astype(jnp.float32)
        backward = jnp.dot(cotangent[:, start_col:start_col + col_width], down_weight[:, start_col:start_col + col_width].T, preferred_element_type=jnp.float32)
        back_total = back_total + backward.astype(jnp.bfloat16).astype(jnp.float32)
    hidden_next = hidden_total.astype(jnp.bfloat16)
    acts_next = squared_relu(hidden_next)
    output_next = jnp.dot(acts_next, down_weight, preferred_element_type=jnp.float32).astype(jnp.bfloat16)
    hidden_saved = hidden_prev.astype(jnp.float32)
    acts_prev = squared_relu(hidden_prev)
    hidden_grad = (back_total * 2.0 * jax.nn.relu(hidden_saved)).astype(jnp.bfloat16)
    input_grad = jnp.dot(hidden_grad, up_weight.T, preferred_element_type=jnp.float32).astype(jnp.bfloat16)
    up_accum_out = up_accum + jnp.dot(inputs_prev.T, hidden_grad, preferred_element_type=jnp.float32)
    down_accum_out = down_accum + jnp.dot(acts_prev.T, cotangent, preferred_element_type=jnp.float32)
    return (output_next, hidden_next, input_grad, up_accum_out, down_accum_out)
```

```python
import jax
import jax.numpy as jnp
from jax import lax
from jax.experimental import pallas as pl
from jax.experimental.pallas import tpu as pltpu
from jax.sharding import PartitionSpec as P

BF = jnp.bfloat16
F32 = jnp.float32
MESH = pl.DeviceIdType.MESH

NZ, NY, NX = 8, 4, 4
N_SEMS = 144


def dot(a, b, ca, cb):
    return lax.dot_general(a, b, (((ca,), (cb,)), ((), ())), preferred_element_type=F32)


def relu(v):
    return jnp.maximum(v, 0.0)


class Copies:
    def __init__(self, send, recv):
        self.send, self.recv, self.count, self.always = send, recv, 0, []

    def slot(self):
        self.count += 1
        assert self.count <= N_SEMS
        return self.count - 1

    def at(self, slot, src, dst, to):
        return pltpu.make_async_remote_copy(
            src_ref=src,
            dst_ref=dst,
            send_sem=self.send.at[slot],
            recv_sem=self.recv.at[slot],
            device_id=to,
            device_id_type=MESH,
        )

    def make(self, src, dst, to):
        made = self.at(self.slot(), src, dst, to)
        self.always.append(made)
        return made


class RingGather:
    def __init__(self, copies, me, block, halves, to, own=None):
        up, down = lax.rem(me + 1, 4), lax.rem(me + 3, 4)
        source = block(me) if own is None else own
        self.to_up = copies.make(source, block(me), to(up))
        self.to_down = copies.make(source, block(me), to(down))
        self.on_up = copies.make(halves(down)[0], halves(down)[0], to(up))
        self.on_down = copies.make(halves(up)[1], halves(up)[1], to(down))

    def start(self):
        self.to_up.start()
        self.to_down.start()

    def middle(self):
        self.to_up.wait_recv()
        self.on_up.start()
        self.to_down.wait_recv()
        self.on_down.start()

    def end(self):
        self.on_up.wait_recv()
        self.on_down.wait_recv()


class RingReduce:
    def __init__(self, copies, me, block, halves, to, bufs):
        up, down, far = lax.rem(me + 1, 4), lax.rem(me + 3, 4), lax.rem(me + 2, 4)
        self.half_up, self.half_down, self.full_up, self.full_down = bufs
        self.far_up = copies.make(halves(far)[0], self.half_up, to(up))
        self.far_down = copies.make(halves(far)[1], self.half_down, to(down))
        self.near_up = copies.make(block(up), self.full_up, to(up))
        self.near_down = copies.make(block(down), self.full_down, to(down))
        self.sum_up, self.sum_down, self.mine = halves(up)[0], halves(down)[1], block(me)

    def start(self):
        self.far_up.start()
        self.far_down.start()

    def middle(self):
        self.far_up.wait_recv()
        add_into(self.sum_up, self.half_up)
        self.far_down.wait_recv()
        add_into(self.sum_down, self.half_down)
        self.near_up.start()
        self.near_down.start()

    def end(self):
        self.near_up.wait_recv()
        self.near_down.wait_recv()
        return (
            self.mine[...].astype(F32)
            + self.full_up[...].astype(F32)
            + self.full_down[...].astype(F32)
        )


def add_into(total, term):
    total[...] = (total[...].astype(F32) + term[...].astype(F32)).astype(BF)


def line_order(ready, hop=5.1, each=2.8):
    orders = []
    for plane in range(NZ):
        steps = []
        for way in (0, 1):
            for weight in (0, 1):
                for turn in range(NZ - 1):
                    dest = NZ - 1 - turn if way == 0 else turn
                    far = plane if way == 0 else NZ - 1 - plane
                    if (dest > plane) if way == 0 else (dest < plane):
                        begin = max(ready[1], ready[weight])
                        if weight == 1:
                            begin = ready[1]
                        else:
                            begin = max(ready[0], ready[1] + each * (NZ - 1))
                        at = begin + hop * far + each * turn if far else ready[weight]
                        steps.append((at, turn, way, weight, dest))
        orders.append(sorted(steps))
    return orders


def kernel(
    xn, xp, ct, hp, upw, dnw, upa, dna,
    out, hn_out, ig, ua, da,
    tok, ut, wg, hps, hpf, apt, hpo, hpi, hns, an, hg, hgt, rsb, sa, sb,
    a1u, a1d, a2u, a2d, a3u, a3d, a4u, a4d, b1u, b1d, b2u, b2d, b3u, b3d, b4u, b4d,
    hng, grd, rr, rl, fg, fr, send, recv,
):
    r, f, t = lax.axis_index("rep"), lax.axis_index("fs"), lax.axis_index("tp")
    z, y, x, c = f // NY, lax.rem(f, NY), t // 2, lax.rem(t, 2)
    big_z = r * NZ + z

    def at_x(i):
        return (r, f, i * 2 + c)

    def at_y(j):
        return (r, z * NY + j, t)

    def at_big_z(k):
        return (k // NZ, lax.rem(k, NZ) * NY + y, t)

    partner = (r, f, x * 2 + 1 - c)
    z_up, z_down = at_big_z(lax.rem(big_z + 1, 2 * NZ)), at_big_z(lax.rem(big_z + 2 * NZ - 1, 2 * NZ))
    xs = [lax.rem(x + k, NX) for k in (1, 3, 2)]
    ys = [lax.rem(y + k, NY) for k in (1, 3, 2)]

    barrier = pltpu.get_barrier_semaphore()
    peers = [partner, z_up, z_down] + [at_x(i) for i in xs] + [at_y(j) for j in ys]
    for peer in peers:
        pl.semaphore_signal(barrier, inc=1, device_id=peer, device_id_type=MESH)

    copies = Copies(send, recv)

    up_t = upw[...].astype(F32).T.astype(BF)
    ut[...] = up_t.reshape(4, 64, 256)
    for k, ref in enumerate((xn, ct, xp)):
        tok[k, x, y] = ref[...]
    pl.semaphore_wait(barrier, len(peers))

    spread = []
    for w, source in ((1, dnw), (0, ut)):
        for i in xs:
            spread.append(copies.make(source.at[i], wg.at[w, x, z], at_x(i)))
    for s in spread:
        s.start()
    wg[1, x, z] = dnw[x]
    wg[0, x, z] = ut[x]

    first_a, first_b, second_a, second_b = {}, {}, {}, {}
    for k, ref in ((1, ct), (0, xn), (2, xp)):
        first_a[k] = RingGather(
            copies, x,
            lambda i, k=k: tok.at[k, i, y, 0:64],
            lambda i, k=k: (tok.at[k, i, y, 0:32], tok.at[k, i, y, 32:64]),
            at_x, ref.at[0:64],
        )
        first_b[k] = RingGather(
            copies, y,
            lambda j, k=k: tok.at[k, x, j, 64:128],
            lambda j, k=k: (tok.at[k, x, j, 64:96], tok.at[k, x, j, 96:128]),
            at_y, ref.at[64:128],
        )
        second_a[k] = RingGather(
            copies, y,
            lambda j, k=k: tok.at[k, :, j, 0:64],
            lambda j, k=k: (tok.at[k, 0:2, j, 0:64], tok.at[k, 2:4, j, 0:64]),
            at_y,
        )
        second_b[k] = RingGather(
            copies, x,
            lambda i, k=k: tok.at[k, i, :, 64:128],
            lambda i, k=k: (tok.at[k, i, 0:2, 64:128], tok.at[k, i, 2:4, 64:128]),
            at_x,
        )
    for k in (1, 0, 2):
        first_a[k].start()
        first_b[k].start()

    lane = lax.broadcasted_iota(jnp.int32, (128, 128), 1)
    low = lane < 64
    odd = lax.rem(x, 2) == 1
    for j in range(NY):
        for m in range(2):
            off = 1024 * (4 * c + 2 * m) + 256 * j + 128 * (x // 2)
            one = hp[:, pl.ds(pl.multiple_of(off, 128), 128)].astype(F32)
            two = hp[:, pl.ds(pl.multiple_of(off + 1024, 128), 128)].astype(F32)
            left = jnp.where(odd, pltpu.roll(one, 64, axis=1), one)
            right = jnp.where(odd, two, pltpu.roll(two, 64, axis=1))
            hps[j, :, 128 * m:128 * m + 128] = jnp.where(low, left, right).astype(BF)
    hpf[c, y] = hps[y]

    for s in spread:
        s.wait_recv()
    gather_z = {}
    for w, rights, lefts in ((1, 3, 4), (0, 4, 3)):
        for way, steps, to in ((0, rights, z_up), (1, lefts, z_down)):
            made = []
            for s in range(steps):
                piece = lax.rem(z + (NZ - s if way == 0 else s), NZ)
                made.append(copies.make(wg.at[w, :, piece], wg.at[w, :, piece], to))
            gather_z[w, way] = made

    def step_z(s):
        for w in (1, 0):
            for way in (0, 1):
                made = gather_z[w, way]
                if 1 <= s <= len(made):
                    made[s - 1].wait_recv()
                if s < len(made):
                    made[s].start()

    step_z(0)
    hp_sends = [copies.make(hps.at[j], hpf.at[c, y], at_y(j)) for j in ys]
    for s in hp_sends:
        s.start()

    for k in (1, 0, 2):
        first_a[k].middle()
        first_b[k].middle()
    for k in (1, 0, 2):
        first_a[k].end()
        first_b[k].end()
        second_a[k].start()
        second_b[k].start()
    for s in hp_sends:
        s.wait_recv()
    hp_pair = copies.make(hpf.at[c], hpf.at[c], partner)
    hp_pair.start()
    step_z(1)
    second_a[1].middle()
    second_b[1].middle()
    second_a[0].middle()
    second_b[0].middle()

    hp_pair.wait_recv()
    for h in range(2):
        for j in range(NY):
            v = relu(hpf[h, j].astype(F32))
            apt[256 * h:256 * h + 256, 128 * j:128 * j + 128] = (
                (v * v).astype(BF).astype(F32).T.astype(BF)
            )
    step_z(2)
    second_a[1].end()
    second_b[1].end()
    second_a[2].middle()
    second_b[2].middle()

    def partial_gradient(w, left, k):
        def body(i, carry):
            right = tok[k, i].reshape(512, 256)
            for h in range(2):
                got = dot(left[256 * h:256 * h + 256, :], right, 1, 0).astype(BF)
                grd[w, i, 4 * h:4 * h + 4] = got.reshape(4, 64, 256)
            return carry

        lax.fori_loop(0, NX, body, 0)

    partial_gradient(1, apt, 1)
    step_z(3)

    base_line = {}
    for way in (0, 1):
        for w in (0, 1):
            base_line[way, w] = [copies.slot() for _ in range(NZ)]
    line_bufs = (rr, rl)

    def line_copy(plane, way, w, dest):
        buf = line_bufs[way]
        first = plane == (0 if way == 0 else NZ - 1)
        source = grd.at[w, :, dest] if first else buf.at[w, dest]
        to = (r, f + NY if way == 0 else f - NY, t)
        return copies.at(base_line[way, w][dest], source, buf.at[w, dest], to), first

    def line_step(plane, way, w, dest):
        made, first = line_copy(plane, way, w, dest)
        if not first:
            made.wait_recv()
            buf = line_bufs[way]

            def body(i, carry):
                buf[w, dest, i] = (
                    buf[w, dest, i].astype(F32) + grd[w, i, dest].astype(F32)
                ).astype(BF)
                return carry

            lax.fori_loop(0, NX, body, 0)
        made.start()

    orders = line_order((34.0, 22.0))
    done = [0] * NZ

    def line_until(time, weights=(0, 1)):
        for plane in range(NZ):
            todo = []
            while done[plane] < len(orders[plane]) and orders[plane][done[plane]][0] <= time:
                todo.append(orders[plane][done[plane]])
                done[plane] += 1
            if todo:

                @pl.when(z == plane)
                def _():
                    for _, _, way, w, dest in todo:
                        line_step(plane, way, w, dest)

    line_until(24.0)
    second_a[0].end()
    second_b[0].end()
    step_z(4)

    def partial_hidden(q, w):
        def body(j, carry):
            for h in range(2):
                total = None
                for i in range(NX):
                    part = dot(
                        tok[q, i, pl.ds(2 * j, 2)].reshape(256, 256),
                        wg[w, i, 4 * h:4 * h + 4].reshape(256, 256),
                        1, 1,
                    )
                    total = part if total is None else total + part
                hpo[q, h, pl.ds(2 * j, 2)] = total.astype(BF).reshape(2, 128, 256)
            return carry

        lax.fori_loop(0, 2, body, 0)

    pair = [copies.make(hpo.at[q], hpi.at[q], partner) for q in range(2)]
    partial_hidden(1, 1)
    pair[1].start()
    partial_hidden(0, 0)
    pair[0].start()
    pair[1].wait_recv()
    for h in range(2):
        for j in range(NY):
            back = hpo[1, h, j].astype(F32) + hpi[1, h, j].astype(F32)
            grad = (back * 2.0 * relu(hpf[h, j].astype(F32))).astype(BF)
            hg[h, j] = grad
            hgt[256 * h:256 * h + 256, 128 * j:128 * j + 128] = grad.astype(F32).T.astype(BF)
    pair[0].wait_recv()
    for h in range(2):
        for j in range(NY):
            hidden = (hpo[0, h, j].astype(F32) + hpi[0, h, j].astype(F32)).astype(BF)
            hns[h, j] = hidden
            v = relu(hidden.astype(F32))
            an[h, j] = (v * v).astype(BF)

    second_a[2].end()
    second_b[2].end()
    partial_gradient(0, hgt, 2)
    line_until(34.0)

    hn_sends = [copies.make(hns.at[c, j], hng.at[c, x, y], at_y(j)) for j in ys]
    for s in hn_sends:
        s.start()
    hng[c, x, y] = hns[c, y]

    def partial_output(q, left, w):
        def body(i, carry):
            for j in range(2):
                total = None
                for h in range(2):
                    part = dot(
                        left[h, 2 * j:2 * j + 2].reshape(256, 256),
                        wg[w, i, 4 * h:4 * h + 4].reshape(256, 256),
                        1, 0,
                    )
                    total = part if total is None else total + part
                rsb[q, i, 2 * j:2 * j + 2] = total.astype(BF).reshape(2, 128, 256)
            return carry

        lax.fori_loop(0, NX, body, 0)

    partial_output(0, an, 1)
    partial_output(1, hg, 0)

    reduce_a1 = RingReduce(
        copies, x,
        lambda i: rsb.at[:, i, :, 0:64],
        lambda i: (rsb.at[:, i, 0:2, 0:64], rsb.at[:, i, 2:4, 0:64]),
        at_x, (a1u, a1d, a2u, a2d),
    )
    reduce_b1 = RingReduce(
        copies, y,
        lambda j: rsb.at[:, :, j, 64:128],
        lambda j: (rsb.at[:, 0:2, j, 64:128], rsb.at[:, 2:4, j, 64:128]),
        at_y, (b1u, b1d, b2u, b2d),
    )
    reduce_a2 = RingReduce(
        copies, y,
        lambda j: sa.at[:, j],
        lambda j: (sa.at[:, j, 0:32], sa.at[:, j, 32:64]),
        at_y, (a3u, a3d, a4u, a4d),
    )
    reduce_b2 = RingReduce(
        copies, x,
        lambda i: sb.at[:, i],
        lambda i: (sb.at[:, i, 0:32], sb.at[:, i, 32:64]),
        at_x, (b3u, b3d, b4u, b4d),
    )
    hn_ring = RingGather(
        copies, x, lambda i: hng.at[c, i], lambda i: (hng.at[c, i, 0:2], hng.at[c, i, 2:4]), at_x
    )
    hn_pair = [copies.make(hng.at[c, i], hng.at[c, i], partner) for i in [x] + xs]

    reduce_a1.start()
    reduce_b1.start()
    line_until(38.0)
    for s in hn_sends:
        s.wait_recv()
    hn_ring.start()
    hn_pair[0].start()
    line_until(41.0)
    reduce_a1.middle()
    reduce_b1.middle()
    line_until(45.0)
    hn_ring.middle()
    hn_pair[1].start()
    hn_pair[2].start()
    line_until(50.0)
    sa[...] = reduce_a1.end().astype(BF)
    sb[...] = reduce_b1.end().astype(BF)
    reduce_a2.start()
    reduce_b2.start()
    line_until(53.0)
    hn_ring.end()
    hn_pair[3].start()
    reduce_a2.middle()
    reduce_b2.middle()
    line_until(57.0)
    total = reduce_a2.end()
    out[0:64, :] = total[0].astype(BF)
    ig[0:64, :] = total[1].astype(BF)
    total = reduce_b2.end()
    out[64:128, :] = total[0].astype(BF)
    ig[64:128, :] = total[1].astype(BF)
    for s in hn_pair:
        s.wait_recv()
    for h in range(2):
        for n in range(2):
            for m in range(2):
                for j in range(NY):
                    one = hng[h, 2 * m, j, :, 128 * n:128 * n + 128].astype(F32)
                    two = hng[h, 2 * m + 1, j, :, 128 * n:128 * n + 128].astype(F32)
                    off = 1024 * (4 * h + 2 * n) + 256 * j + 128 * m
                    hn_out[:, off:off + 128] = jnp.where(
                        low, one, pltpu.roll(two, 64, axis=1)
                    ).astype(BF)
                    hn_out[:, off + 1024:off + 1152] = jnp.where(
                        low, pltpu.roll(one, 64, axis=1), two
                    ).astype(BF)

    line_until(1e9)
    for plane in range(NZ):

        @pl.when(z == plane)
        def _():
            for w in (0, 1):
                if plane > 0:
                    line_copy(plane, 0, w, plane)[0].wait_recv()
                else:
                    rr[w, 0] = jnp.zeros((4, 64, 256), BF)
                if plane < NZ - 1:
                    line_copy(plane, 1, w, plane)[0].wait_recv()
                else:
                    rl[w, NZ - 1] = jnp.zeros((4, 64, 256), BF)

    for w in (0, 1):
        fg[w] = (
            grd[w, :, z].astype(F32) + rr[w, z].astype(F32) + rl[w, z].astype(F32)
        ).astype(BF)
    final = [copies.make(fg.at[w, i], fr.at[w, x], at_x(i)) for w in (0, 1) for i in xs]
    for s in final:
        s.start()
    for w in (0, 1):
        fr[w, x] = fg[w, x]
    for s in final:
        s.wait_recv()
    ua[...] = upa[...] + fr[0].reshape(256, 256).astype(F32).T
    da[...] = dna[...] + fr[1].reshape(256, 256).astype(F32)

    for made in copies.always:
        made.wait_send()
    for plane in range(NZ):

        @pl.when(z == plane)
        def _():
            for _, _, way, w, dest in orders[plane]:
                line_copy(plane, way, w, dest)[0].wait_send()


def local(inputs_next, inputs_prev, hidden_prev, cotangent, up_weight, down_weight, up_accum, down_accum):
    vmem = pl.BlockSpec(memory_space=pltpu.VMEM)
    shapes = [
        (3, 4, 4, 128, 256),
        (4, 64, 256),
        (2, 4, 8, 64, 256),
        (4, 128, 256),
        (2, 4, 128, 256),
        (512, 512),
        (2, 2, 4, 128, 256),
        (2, 2, 4, 128, 256),
        (2, 4, 128, 256),
        (2, 4, 128, 256),
        (2, 4, 128, 256),
        (512, 512),
        (2, 4, 4, 128, 256),
        (2, 4, 64, 256),
        (2, 4, 64, 256),
    ]
    for _ in range(2):
        shapes += [(2, 2, 64, 256)] * 2 + [(2, 4, 64, 256)] * 2
        shapes += [(2, 32, 256)] * 2 + [(2, 64, 256)] * 2
    shapes += [
        (2, 4, 4, 128, 256),
        (2, 4, 8, 64, 256),
        (2, 8, 4, 64, 256),
        (2, 8, 4, 64, 256),
        (2, 4, 64, 256),
        (2, 4, 64, 256),
    ]
    outs = [
        (inputs_next.shape, BF),
        (hidden_prev.shape, BF),
        (inputs_prev.shape, BF),
        (up_accum.shape, F32),
        (down_accum.shape, F32),
    ]
    return pl.pallas_call(
        kernel,
        out_shape=tuple(jax.ShapeDtypeStruct(s, d) for s, d in outs),
        in_specs=[vmem] * 8,
        out_specs=(vmem,) * 5,
        scratch_shapes=[pltpu.VMEM(s, BF) for s in shapes]
        + [pltpu.SemaphoreType.DMA((N_SEMS,)), pltpu.SemaphoreType.DMA((N_SEMS,))],
        compiler_params=pltpu.CompilerParams(
            collective_id=0, has_side_effects=True, vmem_limit_bytes=60 * 1024 * 1024
        ),
    )(
        inputs_next, inputs_prev, cotangent, hidden_prev, up_weight,
        down_weight.reshape(4, 64, 256), up_accum, down_accum,
    )


def solution(mesh):
    rep_fs, fs = ("rep", "fs"), "fs"
    in_specs = (
        P(rep_fs, "tp"),
        P(rep_fs, "tp"),
        P(rep_fs, None),
        P(rep_fs, "tp"),
        P("tp", fs),
        P(fs, "tp"),
        P(("rep", "tp"), fs),
        P(rep_fs, "tp"),
    )
    out_specs = (
        P(rep_fs, "tp"),
        P(rep_fs, None),
        P(rep_fs, "tp"),
        P(("rep", "tp"), fs),
        P(rep_fs, "tp"),
    )
    return jax.shard_map(local, mesh=mesh, in_specs=in_specs, out_specs=out_specs, check_vma=False)
```

```python
import jax
import jax.numpy as jnp
from jax import lax
from jax.experimental import pallas as pl
from jax.experimental.pallas import tpu as pltpu
from jax.sharding import PartitionSpec as P

BF = jnp.bfloat16
F32 = jnp.float32
MESH = pl.DeviceIdType.MESH

NZ, NY, NX = 8, 4, 4
PARTS = 2
VMEM_MAIN = 60 * 1024 * 1024
W0_READY, W1_READY, EARLY = 35.05, 19.5, 5
LATE = (41.0, 44.5, 51.0, 57.0, 60.0, 62.0, 66.0)
N_SEMS = 256


def dot(a, b, ca, cb):
    return lax.dot_general(a, b, (((ca,), (cb,)), ((), ())), preferred_element_type=F32)


def relu(v):
    return jnp.maximum(v, 0.0)


class Copies:
    def __init__(self, send, recv):
        self.send, self.recv, self.count, self.always = send, recv, 0, []

    def slot(self):
        self.count += 1
        assert self.count <= N_SEMS
        return self.count - 1

    def at(self, slot, src, dst, to):
        return pltpu.make_async_remote_copy(
            src_ref=src,
            dst_ref=dst,
            send_sem=self.send.at[slot],
            recv_sem=self.recv.at[slot],
            device_id=to,
            device_id_type=MESH,
        )

    def make(self, src, dst, to):
        made = self.at(self.slot(), src, dst, to)
        self.always.append(made)
        return made


class RingGather:
    def __init__(self, copies, me, block, halves, to):
        up, down = lax.rem(me + 1, 4), lax.rem(me + 3, 4)
        self.to_up = copies.make(block(me), block(me), to(up))
        self.to_down = copies.make(block(me), block(me), to(down))
        self.on_up = copies.make(halves(down)[0], halves(down)[0], to(up))
        self.on_down = copies.make(halves(up)[1], halves(up)[1], to(down))

    def start(self):
        self.to_up.start()
        self.to_down.start()

    def middle(self):
        self.to_up.wait_recv()
        self.on_up.start()
        self.to_down.wait_recv()
        self.on_down.start()

    def end(self):
        self.on_up.wait_recv()
        self.on_down.wait_recv()


class RingReduce:
    def __init__(self, copies, me, block, halves, to, bufs):
        up, down, far = lax.rem(me + 1, 4), lax.rem(me + 3, 4), lax.rem(me + 2, 4)
        self.half_up, self.half_down, self.full_up, self.full_down = bufs
        self.far_up = copies.make(halves(far)[0], self.half_up, to(up))
        self.far_down = copies.make(halves(far)[1], self.half_down, to(down))
        self.near_up = copies.make(block(up), self.full_up, to(up))
        self.near_down = copies.make(block(down), self.full_down, to(down))
        self.sum_up, self.sum_down, self.mine = halves(up)[0], halves(down)[1], block(me)

    def start(self):
        self.far_up.start()
        self.far_down.start()

    def middle(self):
        self.far_up.wait_recv()
        add_into(self.sum_up, self.half_up)
        self.far_down.wait_recv()
        add_into(self.sum_down, self.half_down)
        self.near_up.start()
        self.near_down.start()

    def end(self):
        self.near_up.wait_recv()
        self.near_down.wait_recv()
        return (
            self.mine[...].astype(F32)
            + self.full_up[...].astype(F32)
            + self.full_down[...].astype(F32)
        )


def add_into(total, term):
    total[...] = (total[...].astype(F32) + term[...].astype(F32)).astype(BF)


def line_order(ready, early):
    orders = [[] for _ in range(NZ)]
    for way in (0, 1):
        free = [5.0 + 5.6 * n for n in (3, 3, 3, 4, 4, 4, 4)]
        queue = []
        for turn in range(NZ - 1):
            for part in range(PARTS):
                queue.append((ready[1], 1, turn, part) if turn < early else (ready[0] + 0.01, 1, turn, part))
                queue.append((ready[0], 0, turn, part))
        queue.sort()
        for at, weight, turn, part in queue:
            for hop in range(NZ - 1 - turn):
                plane = hop if way == 0 else NZ - 1 - hop
                dest = NZ - 1 - turn if way == 0 else turn
                begin = max(free[hop], at)
                orders[plane].append((max(at, begin - 0.7) if hop == 0 else at, way, weight, dest, part))
                free[hop] = begin + 2.8 / PARTS
                at = begin + 2.8 / PARTS + 2.5
    return [sorted(o) for o in orders]


def kernel(
    xn_hbm, xp_hbm, ct_hbm, hp_hbm, up_hbm, dn_hbm,
    out, ig, hng, fr,
    hp, upw, dnw, tok, ut, wg, hps, hpf, apt, hpo, hpi, hns, an, hg, hgt, rsb, sa, sb,
    a1u, a1d, a2u, a2d, a3u, a3d, a4u, a4d, b1u, b1d, b2u, b2d, b3u, b3d, b4u, b4d,
    grd, rr, rl, fg, load, send, recv,
):
    r, f, t = lax.axis_index("rep"), lax.axis_index("fs"), lax.axis_index("tp")
    z, y, x, c = f // NY, lax.rem(f, NY), t // 2, lax.rem(t, 2)
    big_z = r * NZ + z

    def at_x(i):
        return (r, f, i * 2 + c)

    def at_y(j):
        return (r, z * NY + j, t)

    def at_big_z(k):
        return (k // NZ, lax.rem(k, NZ) * NY + y, t)

    partner = (r, f, x * 2 + 1 - c)
    z_up, z_down = at_big_z(lax.rem(big_z + 1, 2 * NZ)), at_big_z(lax.rem(big_z + 2 * NZ - 1, 2 * NZ))
    xs = [lax.rem(x + k, NX) for k in (1, 3, 2)]
    ys = [lax.rem(y + k, NY) for k in (1, 3, 2)]

    loads = [
        pltpu.make_async_copy(source, target, load.at[k])
        for k, (source, target) in enumerate((
            (up_hbm, upw), (dn_hbm, dnw), (dn_hbm.at[x], wg.at[1, x, z]),
            (ct_hbm, tok.at[1, x, y]), (xn_hbm, tok.at[0, x, y]), (xp_hbm, tok.at[2, x, y]), (hp_hbm, hp),
        ))
    ]
    for made in loads:
        made.start()
    barrier = pltpu.get_barrier_semaphore()
    peers = [partner, z_up, z_down] + [at_x(i) for i in xs] + [at_y(j) for j in ys]
    for peer in peers:
        pl.semaphore_signal(barrier, inc=1, device_id=peer, device_id_type=MESH)

    copies = Copies(send, recv)

    for made in loads[:3]:
        made.wait()
    ut[...] = upw[...].astype(F32).T.astype(BF).reshape(4, 64, 256)
    wg[0, x, z] = ut[x]
    pl.semaphore_wait(barrier, len(peers))

    steps = []

    def at(time, name, act):
        steps.append((time, len(steps), name, act))

    spread = {}
    for off, i in ((1, xs[0]), (3, xs[1]), (2, xs[2])):
        for w, source in ((1, dnw), (0, ut)):
            spread[w, off] = copies.make(source.at[i], wg.at[w, x, z], at_x(i))
    for off in (1, 3):
        for w in (1, 0):
            spread[w, off].start()
    at(4.65, "spread2", lambda: [spread[w, 2].start() for w in (1, 0)])
    slabs = (x, xs[0], xs[1], xs[2])
    gather_z = {}
    for w in (1, 0):
        for way, to in ((0, z_up), (1, z_down)):
            for s in range(4):
                piece = lax.rem(z + (NZ - s if way == 0 else s), NZ)
                for k, i in enumerate(slabs):
                    slot = copies.slot()
                    gather_z[w, way, s, k] = copies.at(slot, wg.at[w, i, piece], wg.at[w, i, piece], to)

    sends_far = (jnp.logical_and(z >= 3, z <= 6), jnp.logical_and(z >= 1, z <= 4))
    takes_far = (z >= 4, z < 4)

    def step_z(s, k):
        if s == 0:
            if k:
                for w in (1, 0):
                    spread[w, (0, 3, 1, 2)[k]].wait_recv()
            for w in (1, 0):
                for way in (0, 1):
                    gather_z[w, way, 0, k].start()
            return
        for way in (0, 1):
            if s <= 3:
                for w in (1, 0):
                    gather_z[w, way, s - 1, k].wait_recv()
                    if s < 3:
                        gather_z[w, way, s, k].start()
                if s == 3:

                    @pl.when(sends_far[way])
                    def _():
                        for w in (1, 0):
                            gather_z[w, way, 3, k].start()

            else:

                @pl.when(takes_far[way])
                def _():
                    for w in (1, 0):
                        gather_z[w, way, 3, k].wait_recv()

    z_times = (
        (3.2, 6.5, 6.6, 9.9), (7.15, 10.5, 11.1, 13.3), (13.7, 15.1, 16.5, 18.0),
        (19.5, 21.1, 22.5, 24.1), (25.1, 26.5, 28.0, 29.5),
    )
    for s, row in enumerate(z_times):
        for k, time in enumerate(row):
            at(time, f"z{s}{k}", lambda s=s, k=k: step_z(s, k))

    for made in loads[3:6]:
        made.wait()
    token_times = {
        1: ((4.6, 7.25, 10.35), (10.4, 14.95, 18.2), (3.25, 5.8, 8.0), (8.5, 13.2, 16.4)),
        0: ((11.3, 13.9, 16.75), (16.8, 21.4, 24.6), (3.9, 6.45, 8.7), (15.0, 19.6, 22.8)),
        2: ((12.0, 14.6, 17.1), (19.65, 24.5, 27.9), (4.7, 7.2, 9.4), (17.7, 23.1, 26.3)),
    }
    for k, times in token_times.items():
        first = (
            RingGather(
                copies, x,
                lambda i, k=k: tok.at[k, i, y, 0:64],
                lambda i, k=k: (tok.at[k, i, y, 0:32], tok.at[k, i, y, 32:64]),
                at_x,
            ),
            RingGather(
                copies, y,
                lambda j, k=k: tok.at[k, x, j, 64:128],
                lambda j, k=k: (tok.at[k, x, j, 64:96], tok.at[k, x, j, 96:128]),
                at_y,
            ),
        )
        second = (
            RingGather(
                copies, y,
                lambda j, k=k: tok.at[k, :, j, 0:64],
                lambda j, k=k: (tok.at[k, 0:2, j, 0:64], tok.at[k, 2:4, j, 0:64]),
                at_y,
            ),
            RingGather(
                copies, x,
                lambda i, k=k: tok.at[k, i, :, 64:128],
                lambda i, k=k: (tok.at[k, i, 0:2, 64:128], tok.at[k, i, 2:4, 64:128]),
                at_x,
            ),
        )

        for ring, moments, label in zip((first[0], second[0], first[1], second[1]), times, "abcd"):
            for moment, name in zip(moments, ("start", "middle", "end")):
                at(moment, f"t{k}{label}{name}", getattr(ring, name))

    hp_sends = [copies.make(hps.at[j], hpf.at[c, y], at_y(j)) for j in ys]
    hp_pair = copies.make(hpf.at[c], hpf.at[c], partner)

    def hp_first():
        loads[6].wait()
        low = lax.broadcasted_iota(jnp.int32, (128, 128), 1) < 64
        odd = lax.rem(x, 2) == 1
        for j in range(NY):
            for m in range(2):
                off = 1024 * (4 * c + 2 * m) + 256 * j + 128 * (x // 2)
                one = hp[:, pl.ds(pl.multiple_of(off, 128), 128)].astype(F32)
                two = hp[:, pl.ds(pl.multiple_of(off + 1024, 128), 128)].astype(F32)
                left = jnp.where(odd, pltpu.roll(one, 64, axis=1), one)
                right = jnp.where(odd, two, pltpu.roll(two, 64, axis=1))
                hps[j, :, 128 * m:128 * m + 128] = jnp.where(low, left, right).astype(BF)
        hpf[c, y] = hps[y]

    def start_all(made):
        return lambda: [m.start() for m in made]

    def hp_second():
        for m in hp_sends:
            m.wait_recv()
        hp_pair.start()

    def transpose_acts():
        hp_pair.wait_recv()
        for h in range(2):
            for j in range(NY):
                v = relu(hpf[h, j].astype(F32))
                apt[256 * h:256 * h + 256, 128 * j:128 * j + 128] = (v * v).astype(BF).astype(F32).T.astype(BF)

    at(3.4, "hp_first", hp_first)
    at(7.5, "hp_send", start_all(hp_sends))
    at(13.0, "hp_second", hp_second)
    at(14.7, "acts_prev", transpose_acts)

    def partial_gradient(w, left, k):
        def body(i, carry):
            right = tok[k, i].reshape(512, 256)
            for h in range(2):
                got = dot(left[256 * h:256 * h + 256, :], right, 1, 0).astype(BF)
                grd[w, i, 4 * h:4 * h + 4] = got.reshape(4, 64, 256)
            return carry

        lax.fori_loop(0, NX, body, 0)

    at(18.25, "grad1", lambda: partial_gradient(1, apt, 1))

    line_slots = {
        (way, w, part): [copies.slot() for _ in range(NZ)]
        for way in (0, 1) for w in (0, 1) for part in range(PARTS)
    }
    line_bufs = (rr, rl)
    size = NX // PARTS

    def line_copy(plane, way, w, dest, part):
        buf = line_bufs[way]
        first = plane == (0 if way == 0 else NZ - 1)
        span = pl.ds(part * size, size)
        source = grd.at[w, span, dest] if first else buf.at[w, dest, span]
        to = (r, f + NY if way == 0 else f - NY, t)
        return copies.at(line_slots[way, w, part][dest], source, buf.at[w, dest, span], to), first

    def line_step(plane, way, w, dest, part):
        made, first = line_copy(plane, way, w, dest, part)
        if not first:
            made.wait_recv()
            buf = line_bufs[way]
            for i in range(part * size, part * size + size):
                add_into(buf.at[w, dest, i], grd.at[w, i, dest])
        made.start()

    orders = line_order((W0_READY, W1_READY), EARLY)
    done = [0] * NZ

    def line_until(time):
        for plane in range(NZ):
            todo = []
            while done[plane] < len(orders[plane]) and orders[plane][done[plane]][0] <= time:
                todo.append(orders[plane][done[plane]])
                done[plane] += 1
            if todo:

                @pl.when(z == plane)
                def _():
                    for _, *step in todo:
                        line_step(plane, *step)

    def partial_hidden(q, w):
        def body(j, carry):
            for h in range(2):
                total = None
                for i in range(NX):
                    part = dot(
                        tok[q, i, pl.ds(2 * j, 2)].reshape(256, 256),
                        wg[w, i, 4 * h:4 * h + 4].reshape(256, 256),
                        1, 1,
                    )
                    total = part if total is None else total + part
                hpo[q, h, pl.ds(2 * j, 2)] = total.astype(BF).reshape(2, 128, 256)
            return carry

        lax.fori_loop(0, 2, body, 0)

    pair = [copies.make(hpo.at[q], hpi.at[q], partner) for q in range(2)]

    def hidden_sums():
        partial_hidden(1, 1)
        pair[1].start()
        partial_hidden(0, 0)
        pair[0].start()

    def hidden_gradient():
        pair[1].wait_recv()
        for h in range(2):
            for j in range(NY):
                back = hpo[1, h, j].astype(F32) + hpi[1, h, j].astype(F32)
                grad = (back * 2.0 * relu(hpf[h, j].astype(F32))).astype(BF)
                hg[h, j] = grad
                hgt[256 * h:256 * h + 256, 128 * j:128 * j + 128] = grad.astype(F32).T.astype(BF)

    def hidden_acts():
        pair[0].wait_recv()
        for h in range(2):
            for j in range(NY):
                hidden = (hpo[0, h, j].astype(F32) + hpi[0, h, j].astype(F32)).astype(BF)
                hns[h, j] = hidden
                v = relu(hidden.astype(F32))
                an[h, j] = (v * v).astype(BF)

    hn_sends = [copies.make(hns.at[c, j], hng.at[c, x, y], at_y(j)) for j in ys]
    hn_ring = RingGather(
        copies, x, lambda i: hng.at[c, i], lambda i: (hng.at[c, i, 0:2], hng.at[c, i, 2:4]), at_x
    )
    hn_pair = [copies.make(hng.at[c, i], hng.at[c, i], partner) for i in [x] + xs]

    def hn_first():
        for m in hn_sends:
            m.start()
        hng[c, x, y] = hns[c, y]

    def hn_second():
        for m in hn_sends:
            m.wait_recv()
        hn_ring.start()
        hn_pair[0].start()

    def hn_third():
        hn_ring.middle()
        hn_pair[1].start()
        hn_pair[2].start()

    def hn_fourth():
        hn_ring.end()
        hn_pair[3].start()

    def partial_output(q, left, w):
        def body(i, carry):
            for j in range(2):
                total = None
                for h in range(2):
                    part = dot(
                        left[h, 2 * j:2 * j + 2].reshape(256, 256),
                        wg[w, i, 4 * h:4 * h + 4].reshape(256, 256),
                        1, 0,
                    )
                    total = part if total is None else total + part
                rsb[q, i, 2 * j:2 * j + 2] = total.astype(BF).reshape(2, 128, 256)
            return carry

        lax.fori_loop(0, NX, body, 0)

    reduce_a1 = RingReduce(
        copies, x,
        lambda i: rsb.at[:, i, :, 0:64],
        lambda i: (rsb.at[:, i, 0:2, 0:64], rsb.at[:, i, 2:4, 0:64]),
        at_x, (a1u, a1d, a2u, a2d),
    )
    reduce_b1 = RingReduce(
        copies, y,
        lambda j: rsb.at[:, :, j, 64:128],
        lambda j: (rsb.at[:, 0:2, j, 64:128], rsb.at[:, 2:4, j, 64:128]),
        at_y, (b1u, b1d, b2u, b2d),
    )
    reduce_a2 = RingReduce(
        copies, y,
        lambda j: sa.at[:, j],
        lambda j: (sa.at[:, j, 0:32], sa.at[:, j, 32:64]),
        at_y, (a3u, a3d, a4u, a4d),
    )
    reduce_b2 = RingReduce(
        copies, x,
        lambda i: sb.at[:, i],
        lambda i: (sb.at[:, i, 0:32], sb.at[:, i, 32:64]),
        at_x, (b3u, b3d, b4u, b4d),
    )
    def outputs():
        partial_output(0, an, 1)
        partial_output(1, hg, 0)
        reduce_a1.start()
        reduce_b1.start()

    def reduce_second():
        reduce_a1.middle()
        reduce_b1.middle()

    def reduce_third():
        sa[...] = reduce_a1.end().astype(BF)
        reduce_a2.start()
        sb[...] = reduce_b1.end().astype(BF)
        reduce_b2.start()

    def reduce_fourth():
        reduce_a2.middle()
        reduce_b2.middle()

    def reduce_last():
        for rows, ring in ((slice(0, 64), reduce_a2), (slice(64, 128), reduce_b2)):
            total = ring.end()
            out[rows, :] = total[0].astype(BF)
            ig[rows, :] = total[1].astype(BF)

    at(29.9, "hidden", hidden_sums)
    at(32.0, "hidden_grad", hidden_gradient)
    at(33.4, "hidden_acts", hidden_acts)
    at(33.6, "hn1", hn_first)
    at(33.8, "grad0", lambda: partial_gradient(0, hgt, 2))
    at(35.1, "outputs", outputs)
    for time, name, act in zip(
        LATE, ("hn2", "rs2", "hn3", "rs3", "hn4", "rs4", "rs5"),
        (hn_second, reduce_second, hn_third, reduce_third, hn_fourth, reduce_fourth, reduce_last),
    ):
        at(time, name, act)

    for time, _, name, act in sorted(steps, key=lambda step: step[:2]):
        with jax.named_scope(f"line_{name}"):
            line_until(time)
        with jax.named_scope(name):
            act()
    with jax.named_scope("line_rest"):
        line_until(1e9)

    def line_end(w):
        for plane in range(NZ):

            @pl.when(z == plane)
            def _():
                for way, buf, outer in ((0, rr, 0), (1, rl, NZ - 1)):
                    if plane == outer:
                        buf[w, plane] = jnp.zeros((4, 64, 256), BF)
                    else:
                        for part in range(PARTS):
                            line_copy(plane, way, w, plane, part)[0].wait_recv()

        fg[w] = (
            grd[w, :, z].astype(F32) + rr[w, z].astype(F32) + rl[w, z].astype(F32)
        ).astype(BF)
        final = [copies.make(fg.at[w, i], fr.at[w, x], at_x(i)) for i in xs]
        for s in final:
            s.start()
        fr[w, x] = fg[w, x]
        return final

    with jax.named_scope("line_end"):
        final = line_end(1) + line_end(0)
    with jax.named_scope("final_wait"):
        for s in hn_pair + final:
            s.wait_recv()

    for made in copies.always:
        made.wait_send()
    for way in (0, 1):
        for w in (0, 1):
            for k in range(4):
                for s in range(3):
                    gather_z[w, way, s, k].wait_send()

        @pl.when(sends_far[way])
        def _():
            for w in (0, 1):
                for k in range(4):
                    gather_z[w, way, 3, k].wait_send()

    for plane in range(NZ):

        @pl.when(z == plane)
        def _():
            for _, *step in orders[plane]:
                line_copy(plane, *step)[0].wait_send()


def finish(raw_out, raw_ig, hng, fr, upa, dna, out, hn_out, ig, ua, da):
    @pl.when(pl.program_id(0) == 0)
    def _():
        out[...] = raw_out[...]
        ig[...] = raw_ig[...]
        ua[...] = upa[...] + fr[0].reshape(256, 256).astype(F32).T
        da[...] = dna[...] + fr[1].reshape(256, 256).astype(F32)

    low = lax.broadcasted_iota(jnp.int32, (128, 128), 1) < 64
    for m in range(2):
        for j in range(NY):
            one = hng[0, 2 * m, j].astype(F32)
            two = hng[0, 2 * m + 1, j].astype(F32)
            off = 256 * j + 128 * m
            hn_out[:, off:off + 128] = jnp.where(low, one, pltpu.roll(two, 64, axis=1)).astype(BF)
            hn_out[:, off + 1024:off + 1152] = jnp.where(low, pltpu.roll(one, 64, axis=1), two).astype(BF)


def local(inputs_next, inputs_prev, hidden_prev, cotangent, up_weight, down_weight, up_accum, down_accum):
    vmem = pl.BlockSpec(memory_space=pltpu.VMEM)
    shapes = [
        (128, 8192),
        (256, 256),
        (4, 64, 256),
        (3, 4, 4, 128, 256),
        (4, 64, 256),
        (2, 4, 8, 64, 256),
        (4, 128, 256),
        (2, 4, 128, 256),
        (512, 512),
        (2, 2, 4, 128, 256),
        (2, 2, 4, 128, 256),
        (2, 4, 128, 256),
        (2, 4, 128, 256),
        (2, 4, 128, 256),
        (512, 512),
        (2, 4, 4, 128, 256),
        (2, 4, 64, 256),
        (2, 4, 64, 256),
    ]
    for _ in range(2):
        shapes += [(2, 2, 64, 256)] * 2 + [(2, 4, 64, 256)] * 2
        shapes += [(2, 32, 256)] * 2 + [(2, 64, 256)] * 2
    shapes += [
        (2, 4, 8, 64, 256),
        (2, 8, 4, 64, 256),
        (2, 8, 4, 64, 256),
        (2, 4, 64, 256),
    ]
    raw = [(128, 256), (128, 256), (2, 4, 4, 128, 256), (2, 4, 64, 256)]
    results = pl.pallas_call(
        kernel,
        out_shape=tuple(pltpu.VMEM(s, BF) for s in raw),
        in_specs=[pl.BlockSpec(memory_space=pltpu.HBM)] * 6,
        out_specs=(vmem,) * 4,
        scratch_shapes=[pltpu.VMEM(s, BF) for s in shapes]
        + [pltpu.SemaphoreType.DMA((7,)), pltpu.SemaphoreType.DMA((N_SEMS,)), pltpu.SemaphoreType.DMA((N_SEMS,))],
        compiler_params=pltpu.CompilerParams(
            collective_id=0, has_side_effects=True, vmem_limit_bytes=VMEM_MAIN
        ),
    )(inputs_next, inputs_prev, cotangent, hidden_prev, up_weight, down_weight.reshape(4, 64, 256))

    outs = [
        (inputs_next.shape, BF, (128, 256)),
        (hidden_prev.shape, BF, (128, 2048)),
        (inputs_prev.shape, BF, (128, 256)),
        (up_accum.shape, F32, (256, 256)),
        (down_accum.shape, F32, (256, 256)),
    ]
    whole = pl.BlockSpec((128, 256), lambda i: (0, 0))
    square = pl.BlockSpec((256, 256), lambda i: (0, 0))
    return pl.pallas_call(
        finish,
        grid=(4,),
        out_shape=tuple(jax.ShapeDtypeStruct(s, d) for s, d, _ in outs),
        in_specs=[
            whole, whole,
            pl.BlockSpec((1, 4, 4, 128, 128), lambda i: (i // 2, 0, 0, 0, i % 2)),
            pl.BlockSpec((2, 4, 64, 256), lambda i: (0, 0, 0, 0)),
            square, square,
        ],
        out_specs=tuple(
            pl.BlockSpec(b, (lambda i: (0, i)) if n == 1 else (lambda i: (0, 0)))
            for n, (_, _, b) in enumerate(outs)
        ),
        compiler_params=pltpu.CompilerParams(vmem_limit_bytes=16 * 1024 * 1024),
    )(*results, up_accum, down_accum)


def solution(mesh):
    rep_fs, fs = ("rep", "fs"), "fs"
    in_specs = (
        P(rep_fs, "tp"),
        P(rep_fs, "tp"),
        P(rep_fs, None),
        P(rep_fs, "tp"),
        P("tp", fs),
        P(fs, "tp"),
        P(("rep", "tp"), fs),
        P(rep_fs, "tp"),
    )
    out_specs = (
        P(rep_fs, "tp"),
        P(rep_fs, None),
        P(rep_fs, "tp"),
        P(("rep", "tp"), fs),
        P(rep_fs, "tp"),
    )
    return jax.shard_map(local, mesh=mesh, in_specs=in_specs, out_specs=out_specs, check_vma=False)
```

```python
import math

import jax
import jax.numpy as jnp
from jax import lax
from jax.experimental import pallas as pl
from jax.experimental.pallas import tpu as pltpu
from jax.sharding import PartitionSpec as P

BF = jnp.bfloat16
F32 = jnp.float32
MESH = pl.DeviceIdType.MESH

NZ, NY, NX = 8, 4, 4
PARTS = 2
LATER = 0.0
VMEM_MAIN = 60 * 1024 * 1024
W0_READY, W1_READY, EARLY, HOP, LEAD = 35.05, 22.5, 5, 2.5, 0.7
LATE = (40.0, 43.0, 48.0, 52.0, 55.0, 56.0, 61.0)
VMEM_MAIN = 60 * 1024 * 1024
W0_READY, W1_READY, EARLY = 35.05, 19.5, 5
LATE = (40.0, 43.0, 48.0, 52.0, 55.0, 56.0, 61.0)
N_RECV, N_SEND = 139, 19


def dot(a, b, ca, cb):
    return lax.dot_general(a, b, (((ca,), (cb,)), ((), ())), preferred_element_type=F32)


def relu(v):
    return jnp.maximum(v, 0.0)


class Copies:
    def __init__(self, send, recv):
        self.send, self.recv, self.count, self.groups, self.group = send, recv, 0, [], 0

    def slots(self, n):
        self.count += n
        assert self.count <= N_RECV
        return self.count - n

    def begin(self):
        self.groups.append(0)
        self.group = len(self.groups) - 1
        return self.group

    def at(self, slot, group, src, dst, to):
        return pltpu.make_async_remote_copy(
            src_ref=src,
            dst_ref=dst,
            send_sem=self.send.at[group],
            recv_sem=self.recv.at[slot],
            device_id=to,
            device_id_type=MESH,
        )

    def make(self, src, dst, to):
        self.groups[self.group] += math.prod(src.shape)
        return self.at(self.slots(1), self.group, src, dst, to)

    def wait_sent(self, group, size, ref):
        part = ref.at[:, 0:size // 128]
        pltpu.make_async_copy(part, part, self.send.at[group]).wait()


class RingGather:
    def __init__(self, copies, me, block, halves, to):
        up, down = lax.rem(me + 1, 4), lax.rem(me + 3, 4)
        self.to_up = copies.make(block(me), block(me), to(up))
        self.to_down = copies.make(block(me), block(me), to(down))
        self.on_up = copies.make(halves(down)[0], halves(down)[0], to(up))
        self.on_down = copies.make(halves(up)[1], halves(up)[1], to(down))

    def start(self):
        self.to_up.start()
        self.to_down.start()

    def middle(self):
        self.to_up.wait_recv()
        self.on_up.start()
        self.to_down.wait_recv()
        self.on_down.start()

    def end(self):
        self.on_up.wait_recv()
        self.on_down.wait_recv()


class RingReduce:
    def __init__(self, copies, me, block, halves, to, bufs):
        up, down, far = lax.rem(me + 1, 4), lax.rem(me + 3, 4), lax.rem(me + 2, 4)
        self.half_up, self.half_down, self.full_up, self.full_down = bufs
        self.far_up = copies.make(halves(far)[0], self.half_up, to(up))
        self.far_down = copies.make(halves(far)[1], self.half_down, to(down))
        self.near_up = copies.make(block(up), self.full_up, to(up))
        self.near_down = copies.make(block(down), self.full_down, to(down))
        self.sum_up, self.sum_down, self.mine = halves(up)[0], halves(down)[1], block(me)

    def start(self):
        self.far_up.start()
        self.far_down.start()

    def middle(self):
        self.far_up.wait_recv()
        add_into(self.sum_up, self.half_up)
        self.far_down.wait_recv()
        add_into(self.sum_down, self.half_down)
        self.near_up.start()
        self.near_down.start()

    def end(self):
        self.near_up.wait_recv()
        self.near_down.wait_recv()
        return (
            self.mine[...].astype(F32)
            + self.full_up[...].astype(F32)
            + self.full_down[...].astype(F32)
        )


def add_into(total, term):
    total[...] = (total[...].astype(F32) + term[...].astype(F32)).astype(BF)


def line_order(ready, early):
    orders = [[] for _ in range(NZ)]
    for way in (0, 1):
        free = [W1_READY, 26.0, 26.0, 30.0, 30.0, 30.0, 30.0]
        queue = []
        for turn in range(NZ - 1):
            for part in range(PARTS):
                queue.append((ready[1], 1, turn, part) if turn < early else (ready[0] + 0.01, 1, turn, part))
                queue.append((ready[0], 0, turn, part))
        queue.sort()
        for at, weight, turn, part in queue:
            for hop in range(NZ - 1 - turn):
                plane = hop if way == 0 else NZ - 1 - hop
                dest = NZ - 1 - turn if way == 0 else turn
                begin = max(free[hop], at)
                orders[plane].append((max(at, begin - LEAD) if hop == 0 else at, way, weight, dest, part))
                free[hop] = begin + 2.8 / PARTS
                at = begin + 2.8 / PARTS + HOP
    return [sorted(o) for o in orders]


def kernel(
    xn_hbm, xp_hbm, ct_hbm, hp_hbm, up_hbm, dn_hbm,
    out, ig, hng, fr,
    hp, upw, own, tok, wg, hps, hpf, apt, hpo, hpi, hns, an, hg, hgt, rsb, sa, sb,
    a1u, a1d, a2u, a2d, a3u, a3d, a4u, a4d, b1u, b1d, b2u, b2d, b3u, b3d, b4u, b4d,
    grd, line, fg, sums, load, send, recv,
):
    r, f, t = lax.axis_index("rep"), lax.axis_index("fs"), lax.axis_index("tp")
    z, y, x, c = f // NY, lax.rem(f, NY), t // 2, lax.rem(t, 2)
    big_z = r * NZ + z

    def at_x(i):
        return (r, f, i * 2 + c)

    def at_y(j):
        return (r, z * NY + j, t)

    def at_big_z(k):
        return (k // NZ, lax.rem(k, NZ) * NY + y, t)

    partner = (r, f, x * 2 + 1 - c)
    z_up, z_down = at_big_z(lax.rem(big_z + 1, 2 * NZ)), at_big_z(lax.rem(big_z + 2 * NZ - 1, 2 * NZ))
    xs = [lax.rem(x + k, NX) for k in (1, 3, 2)]
    ys = [lax.rem(y + k, NY) for k in (1, 3, 2)]

    loads = [
        pltpu.make_async_copy(source, target, load.at[k])
        for k, (source, target) in enumerate((
            (up_hbm, upw), (dn_hbm, own.at[1]), (dn_hbm.at[x], wg.at[1, x, z]),
            (ct_hbm, tok.at[0, x, y]), (xn_hbm, tok.at[1, x, y]), (xp_hbm, tok.at[2, x, y]), (hp_hbm, hp),
        ))
    ]
    for made in loads:
        made.start()
    barrier = pltpu.get_barrier_semaphore()
    peers = [partner, z_up, z_down] + [at_x(i) for i in xs] + [at_y(j) for j in ys]
    for peer in peers:
        pl.semaphore_signal(barrier, inc=1, device_id=peer, device_id_type=MESH)

    copies = Copies(send, recv)

    for made in loads[:3]:
        made.wait()
    own[0] = upw[...].astype(F32).T.astype(BF).reshape(4, 64, 256)
    wg[0, x, z] = own[0, x]
    with jax.named_scope("barrier"):
        pl.semaphore_wait(barrier, len(peers))

    steps = []

    def at(time, name, act):
        steps.append((time, len(steps), name, act))

    copies.begin()
    spread = {off: copies.make(own.at[:, i], wg.at[:, x, z], at_x(i)) for off, i in ((1, xs[0]), (3, xs[1]), (2, xs[2]))}
    spread[1].start()
    spread[3].start()
    at(4.65, "spread2", lambda: spread[2].start())
    slabs = (x, xs[0], xs[1], xs[2])
    gather_z = {}
    z_group = copies.begin()
    far_groups = (copies.begin(), copies.begin())
    for way, to in ((0, z_up), (1, z_down)):
        for s in range(4):
            piece = lax.rem(z + (NZ - s if way == 0 else s), NZ)
            for k, i in enumerate(slabs):
                place = wg.at[:, i, piece]
                gather_z[way, s, k] = copies.at(
                    copies.slots(1), z_group if s < 3 else far_groups[way], place, place, to
                )

    sends_far = (jnp.logical_and(z >= 3, z <= 6), jnp.logical_and(z >= 1, z <= 4))
    takes_far = (z >= 4, z < 4)

    def begin_z(way, k):
        gather_z[way, 0, k].start()

    def step_z(s, k, way):
        if s <= 3:
            gather_z[way, s - 1, k].wait_recv()
            if s < 3:
                gather_z[way, s, k].start()
            else:
                pl.when(sends_far[way])(lambda: gather_z[way, 3, k].start())
        else:
            pl.when(takes_far[way])(lambda: gather_z[way, 3, k].wait_recv())

    def first_z(k):
        if k:
            spread[(0, 3, 1, 2)[k]].wait_recv()
        begin_z(0, k)
        begin_z(1, k)

    def behind(s):
        return jnp.logical_and(big_z >= 1, big_z <= s)

    def prompt_z(s, k):
        if s <= 3:
            pl.when(jnp.logical_not(behind(s)))(lambda: step_z(s, k, 0))
        else:
            step_z(s, k, 0)
        step_z(s, k, 1)

    def later_z(s, k):
        pl.when(behind(s))(lambda: step_z(s, k, 0))

    z_times = (
        (3.2, 6.5, 6.6, 9.9), (7.15, 10.5, 11.1, 13.3), (13.7, 15.1, 16.5, 18.0),
        (19.5, 21.1, 22.5, 24.1), (25.1, 26.5, 28.0, 29.5),
    )
    for s, row in enumerate(z_times):
        for k, time in enumerate(row):
            if s == 0:
                at(time, f"z{s}{k}", lambda k=k: first_z(k))
            else:
                at(time, f"z{s}{k}", lambda s=s, k=k: prompt_z(s, k))
            if 1 <= s <= 3:
                at(min(time + LATER, 29.8), f"y{s}{k}", lambda s=s, k=k: later_z(s, k))
    for made in loads[3:6]:
        made.wait()
    token_times = {
        (0, 1): ((4.6, 7.25, 10.35), (10.4, 14.95, 18.2), (3.25, 5.8, 8.0), (8.5, 13.2, 16.4)),
        (1, 3): ((11.3, 13.9, 16.75), (16.8, 21.4, 24.6), (3.9, 6.45, 8.7), (15.0, 19.6, 22.8)),
    }
    for (k, end), times in token_times.items():
        copies.begin()
        ks = slice(k, end)
        first = (
            RingGather(
                copies, x,
                lambda i, ks=ks: tok.at[ks, i, y, 0:64],
                lambda i, ks=ks: (tok.at[ks, i, y, 0:32], tok.at[ks, i, y, 32:64]),
                at_x,
            ),
            RingGather(
                copies, y,
                lambda j, ks=ks: tok.at[ks, x, j, 64:128],
                lambda j, ks=ks: (tok.at[ks, x, j, 64:96], tok.at[ks, x, j, 96:128]),
                at_y,
            ),
        )
        second = (
            RingGather(
                copies, y,
                lambda j, ks=ks: tok.at[ks, :, j, 0:64],
                lambda j, ks=ks: (tok.at[ks, 0:2, j, 0:64], tok.at[ks, 2:4, j, 0:64]),
                at_y,
            ),
            RingGather(
                copies, x,
                lambda i, ks=ks: tok.at[ks, i, :, 64:128],
                lambda i, ks=ks: (tok.at[ks, i, 0:2, 64:128], tok.at[ks, i, 2:4, 64:128]),
                at_x,
            ),
        )

        for ring, moments, label in zip((first[0], second[0], first[1], second[1]), times, "abcd"):
            for moment, name in zip(moments, ("start", "middle", "end")):
                at(moment, f"t{k}{label}{name}", getattr(ring, name))

    copies.begin()
    hp_sends = [copies.make(hps.at[j], hpf.at[c, y], at_y(j)) for j in ys]
    hp_pair = copies.make(hpf.at[c], hpf.at[c], partner)

    def hp_first():
        loads[6].wait()
        low = lax.broadcasted_iota(jnp.int32, (128, 128), 1) < 64
        odd = lax.rem(x, 2) == 1
        for j in range(NY):
            for m in range(2):
                off = 1024 * (4 * c + 2 * m) + 256 * j + 128 * (x // 2)
                one = hp[:, pl.ds(pl.multiple_of(off, 128), 128)].astype(F32)
                two = hp[:, pl.ds(pl.multiple_of(off + 1024, 128), 128)].astype(F32)
                left = jnp.where(odd, pltpu.roll(one, 64, axis=1), one)
                right = jnp.where(odd, two, pltpu.roll(two, 64, axis=1))
                hps[j, :, 128 * m:128 * m + 128] = jnp.where(low, left, right).astype(BF)
        hpf[c, y] = hps[y]

    def start_all(made):
        return lambda: [m.start() for m in made]

    def hp_second():
        for m in hp_sends:
            m.wait_recv()
        hp_pair.start()

    def transpose_acts():
        hp_pair.wait_recv()
        for h in range(2):
            for j in range(NY):
                v = relu(hpf[h, j].astype(F32))
                apt[256 * h:256 * h + 256, 128 * j:128 * j + 128] = (v * v).astype(BF).astype(F32).T.astype(BF)

    at(3.4, "hp_first", hp_first)
    at(7.5, "hp_send", start_all(hp_sends))
    at(13.0, "hp_second", hp_second)
    at(14.7, "acts_prev", transpose_acts)

    def partial_gradient(w, left, k):
        def body(i, carry):
            right = tok[k, i].reshape(512, 256)
            for h in range(2):
                got = dot(left[256 * h:256 * h + 256, :], right, 1, 0).astype(BF)
                grd[w, i, 4 * h:4 * h + 4] = got.reshape(4, 64, 256)
            return carry

        lax.fori_loop(0, NX, body, 0)

    at(18.25, "grad1", lambda: partial_gradient(1, apt, 0))

    line_base = copies.slots(2 * PARTS * (NZ + 1))
    line_groups = [copies.begin() for _ in range(NZ)]
    size = NX // PARTS

    def line_copy(way, w, dest, part):
        slot = line_base + (w * PARTS + part) * (NZ + 1) + dest + 1 - way
        place = line.at[way, w, dest, pl.ds(part * size, size)]
        return copies.at(slot, line_groups[0] + dest, place, place, (r, f + NY - 2 * NY * way, t))

    def line_item(way, turn):
        dests = jnp.where(way == 0, NZ - 1 - z, z)
        early = PARTS * jnp.minimum(EARLY, dests)
        late = turn - early - PARTS * dests
        w = jnp.where(jnp.logical_or(turn < early, late >= 0), 1, 0)
        count = jnp.where(turn < early, turn, jnp.where(late < 0, turn - early, early + late))
        nth = count // PARTS
        return w, jnp.where(way == 0, NZ - 1 - nth, nth), lax.rem(count, PARTS)

    orders = line_order((W0_READY, W1_READY), EARLY)
    of_plane = [
        sum((step[1] << n) for n, step in enumerate(order)) for order in orders
    ]

    def for_plane(values):
        found = values[NZ - 1]
        for plane in range(NZ - 1):
            found = jnp.where(z == plane, values[plane], found)
        return found

    ways = for_plane(of_plane)

    def line_body(n, rights):
        way = lax.rem(lax.shift_right_logical(ways, n), 2)
        w, dest, part = line_item(way, jnp.where(way == 0, rights, n - rights))
        made = line_copy(way, w, dest, part)
        inner = jnp.where(way == 0, z > 0, z < NZ - 1)

        @pl.when(inner)
        def _():
            with jax.named_scope("lw"):
                made.wait_recv()

        for i in range(size):
            place = line.at[way, w, dest, part * size + i]
            came = jnp.where(inner, place[...].astype(F32), 0.0)
            place[...] = (came + grd[w, part * size + i, dest].astype(F32)).astype(BF)
        made.start()
        return rights + 1 - way

    line_done = [0, jnp.int32(0), [0] * NZ]

    def line_until(time):
        ends = [sum(step[0] <= time for step in order) for order in orders]
        if ends == line_done[2]:
            return
        end = for_plane(ends)
        line_done[1] = lax.fori_loop(line_done[0], end, line_body, line_done[1])
        line_done[0], line_done[2] = end, ends

    def partial_hidden(q, w):
        def body(j, carry):
            for h in range(2):
                total = None
                for i in range(NX):
                    part = dot(
                        tok[1 - q, i, pl.ds(2 * j, 2)].reshape(256, 256),
                        wg[w, i, 4 * h:4 * h + 4].reshape(256, 256),
                        1, 1,
                    )
                    total = part if total is None else total + part
                hpo[q, h, pl.ds(2 * j, 2)] = total.astype(BF).reshape(2, 128, 256)
            return carry

        lax.fori_loop(0, 2, body, 0)

    copies.begin()
    pair = [copies.make(hpo.at[q], hpi.at[q], partner) for q in range(2)]

    def hidden_sums():
        partial_hidden(1, 1)
        pair[1].start()
        partial_hidden(0, 0)
        pair[0].start()

    def hidden_gradient():
        pair[1].wait_recv()
        for h in range(2):
            for j in range(NY):
                back = hpo[1, h, j].astype(F32) + hpi[1, h, j].astype(F32)
                grad = (back * 2.0 * relu(hpf[h, j].astype(F32))).astype(BF)
                hg[h, j] = grad
                hgt[256 * h:256 * h + 256, 128 * j:128 * j + 128] = grad.astype(F32).T.astype(BF)

    def hidden_acts():
        pair[0].wait_recv()
        for h in range(2):
            for j in range(NY):
                hidden = (hpo[0, h, j].astype(F32) + hpi[0, h, j].astype(F32)).astype(BF)
                hns[h, j] = hidden
                v = relu(hidden.astype(F32))
                an[h, j] = (v * v).astype(BF)

    copies.begin()
    hn_sends = [copies.make(hns.at[c, j], hng.at[c, x, y], at_y(j)) for j in ys]
    hn_ring = RingGather(
        copies, x, lambda i: hng.at[c, i], lambda i: (hng.at[c, i, 0:2], hng.at[c, i, 2:4]), at_x
    )
    hn_pair = [copies.make(hng.at[c, i], hng.at[c, i], partner) for i in [x] + xs]

    hn_own = pltpu.make_async_copy(hns.at[c, y], hng.at[c, x, y], load.at[7])

    def hn_first():
        for m in hn_sends:
            m.start()
        hn_own.start()

    def hn_second():
        hn_own.wait()
        for m in hn_sends:
            m.wait_recv()
        hn_ring.start()
        hn_pair[0].start()

    def hn_third():
        hn_ring.middle()
        hn_pair[1].start()
        hn_pair[2].start()

    def hn_fourth():
        hn_ring.end()
        hn_pair[3].start()

    def partial_output(q, left, w):
        def body(i, carry):
            for j in range(2):
                total = None
                for h in range(2):
                    part = dot(
                        left[h, 2 * j:2 * j + 2].reshape(256, 256),
                        wg[w, i, 4 * h:4 * h + 4].reshape(256, 256),
                        1, 0,
                    )
                    total = part if total is None else total + part
                rsb[q, i, 2 * j:2 * j + 2] = total.astype(BF).reshape(2, 128, 256)
            return carry

        lax.fori_loop(0, NX, body, 0)

    copies.begin()
    reduce_a1 = RingReduce(
        copies, x,
        lambda i: rsb.at[:, i, :, 0:64],
        lambda i: (rsb.at[:, i, 0:2, 0:64], rsb.at[:, i, 2:4, 0:64]),
        at_x, (a1u, a1d, a2u, a2d),
    )
    reduce_b1 = RingReduce(
        copies, y,
        lambda j: rsb.at[:, :, j, 64:128],
        lambda j: (rsb.at[:, 0:2, j, 64:128], rsb.at[:, 2:4, j, 64:128]),
        at_y, (b1u, b1d, b2u, b2d),
    )
    reduce_a2 = RingReduce(
        copies, y,
        lambda j: sa.at[:, j],
        lambda j: (sa.at[:, j, 0:32], sa.at[:, j, 32:64]),
        at_y, (a3u, a3d, a4u, a4d),
    )
    reduce_b2 = RingReduce(
        copies, x,
        lambda i: sb.at[:, i],
        lambda i: (sb.at[:, i, 0:32], sb.at[:, i, 32:64]),
        at_x, (b3u, b3d, b4u, b4d),
    )
    def outputs():
        partial_output(0, an, 1)
        partial_output(1, hg, 0)
        reduce_a1.start()
        reduce_b1.start()

    def reduce_second():
        reduce_a1.middle()
        reduce_b1.middle()

    def reduce_third():
        sa[...] = reduce_a1.end().astype(BF)
        reduce_a2.start()
        sb[...] = reduce_b1.end().astype(BF)
        reduce_b2.start()

    def reduce_fourth():
        reduce_a2.middle()
        reduce_b2.middle()

    results = [
        pltpu.make_async_copy(sums.at[k], ref, load.at[8 + k]) for k, ref in enumerate((out, ig))
    ]

    def reduce_last():
        for rows, ring in ((slice(0, 64), reduce_a2), (slice(64, 128), reduce_b2)):
            total = ring.end()
            sums[0, rows, :] = total[0].astype(BF)
            sums[1, rows, :] = total[1].astype(BF)
        for made in results:
            made.start()

    at(29.9, "hidden", hidden_sums)
    at(32.0, "hidden_grad", hidden_gradient)
    at(33.4, "hidden_acts", hidden_acts)
    at(33.6, "hn1", hn_first)
    at(33.8, "grad0", lambda: partial_gradient(0, hgt, 2))
    at(35.1, "outputs", outputs)
    for time, name, act in zip(
        LATE, ("hn2", "rs2", "hn3", "rs3", "hn4", "rs4", "rs5"),
        (hn_second, reduce_second, hn_third, reduce_third, hn_fourth, reduce_fourth, reduce_last),
    ):
        at(time, name, act)

    for time, _, name, act in sorted(steps, key=lambda step: step[:2]):
        with jax.named_scope(f"line_{name}"):
            line_until(time)
        with jax.named_scope(name):
            act()
    with jax.named_scope("line_rest"):
        line_until(1e9)

    def line_end(w):
        for way, inner in ((0, z > 0), (1, z < NZ - 1)):

            @pl.when(inner)
            def _():
                for part in range(PARTS):
                    line_copy(way, w, z, part).wait_recv()

        fg[w] = (
            grd[w, :, z].astype(F32)
            + jnp.where(z > 0, line[0, w, z].astype(F32), 0.0)
            + jnp.where(z < NZ - 1, line[1, w, z].astype(F32), 0.0)
        ).astype(BF)

    with jax.named_scope("line_end"):
        line_end(1)
        line_end(0)
    copies.begin()
    final = [copies.make(fg.at[:, i], fr.at[:, x], at_x(i)) for i in xs]
    kept = pltpu.make_async_copy(fg.at[:, x], fr.at[:, x], load.at[10])
    for s in final + [kept]:
        s.start()
    results.append(kept)
    with jax.named_scope("final_wait"):
        for s in hn_pair + final:
            s.wait_recv()
        for s in results:
            s.wait()

    with jax.named_scope("sent"):
        for group, total in enumerate(copies.groups):
            if total:
                copies.wait_sent(group, total, hp)
        copies.wait_sent(z_group, 3 * 2 * 4 * 2 * 64 * 256, hp)
        for way in (0, 1):
            pl.when(sends_far[way])(lambda: copies.wait_sent(far_groups[way], 4 * 2 * 64 * 256, hp))

        def line_sent(dest, carry):
            pl.when(dest != z)(lambda: copies.wait_sent(line_groups[0] + dest, 2 * NX * 64 * 256, hp))
            return carry

        lax.fori_loop(0, NZ, line_sent, 0)
    assert len(copies.groups) <= N_SEND


def finish(raw_out, raw_ig, hng, fr, upa, dna, out, hn_out, ig, ua, da):
    @pl.when(pl.program_id(0) == 0)
    def _():
        out[...] = raw_out[...]
        ig[...] = raw_ig[...]
        ua[...] = upa[...] + fr[0].reshape(256, 256).astype(F32).T
        da[...] = dna[...] + fr[1].reshape(256, 256).astype(F32)

    low = lax.broadcasted_iota(jnp.int32, (128, 128), 1) < 64
    for m in range(2):
        for j in range(NY):
            one = hng[0, 2 * m, j].astype(F32)
            two = hng[0, 2 * m + 1, j].astype(F32)
            off = 256 * j + 128 * m
            hn_out[:, off:off + 128] = jnp.where(low, one, pltpu.roll(two, 64, axis=1)).astype(BF)
            hn_out[:, off + 1024:off + 1152] = jnp.where(low, pltpu.roll(one, 64, axis=1), two).astype(BF)


def local(inputs_next, inputs_prev, hidden_prev, cotangent, up_weight, down_weight, up_accum, down_accum):
    vmem = pl.BlockSpec(memory_space=pltpu.VMEM)
    shapes = [
        (128, 8192),
        (256, 256),
        (2, 4, 64, 256),
        (3, 4, 4, 128, 256),
        (2, 4, 8, 64, 256),
        (4, 128, 256),
        (2, 4, 128, 256),
        (512, 512),
        (2, 2, 4, 128, 256),
        (2, 2, 4, 128, 256),
        (2, 4, 128, 256),
        (2, 4, 128, 256),
        (2, 4, 128, 256),
        (512, 512),
        (2, 4, 4, 128, 256),
        (2, 4, 64, 256),
        (2, 4, 64, 256),
    ]
    for _ in range(2):
        shapes += [(2, 2, 64, 256)] * 2 + [(2, 4, 64, 256)] * 2
        shapes += [(2, 32, 256)] * 2 + [(2, 64, 256)] * 2
    shapes += [
        (2, 4, 8, 64, 256),
        (2, 2, 8, 4, 64, 256),
        (2, 4, 64, 256),
        (2, 128, 256),
    ]
    raw = [(128, 256), (128, 256), (2, 4, 4, 128, 256), (2, 4, 64, 256)]
    results = pl.pallas_call(
        kernel,
        out_shape=tuple(pltpu.VMEM(s, BF) for s in raw),
        in_specs=[pl.BlockSpec(memory_space=pltpu.HBM)] * 6,
        out_specs=(pl.BlockSpec(memory_space=pl.ANY),) * 4,
        scratch_shapes=[pltpu.VMEM(s, BF) for s in shapes]
        + [pltpu.SemaphoreType.DMA((11,)), pltpu.SemaphoreType.DMA((N_SEND,)), pltpu.SemaphoreType.DMA((N_RECV,))],
        compiler_params=pltpu.CompilerParams(
            collective_id=0, has_side_effects=True, vmem_limit_bytes=VMEM_MAIN
        ),
    )(inputs_next, inputs_prev, cotangent, hidden_prev, up_weight, down_weight.reshape(4, 64, 256))

    outs = [
        (inputs_next.shape, BF, (128, 256)),
        (hidden_prev.shape, BF, (128, 2048)),
        (inputs_prev.shape, BF, (128, 256)),
        (up_accum.shape, F32, (256, 256)),
        (down_accum.shape, F32, (256, 256)),
    ]
    whole = pl.BlockSpec((128, 256), lambda i: (0, 0))
    square = pl.BlockSpec((256, 256), lambda i: (0, 0))
    return pl.pallas_call(
        finish,
        grid=(4,),
        out_shape=tuple(jax.ShapeDtypeStruct(s, d) for s, d, _ in outs),
        in_specs=[
            whole, whole,
            pl.BlockSpec((1, 4, 4, 128, 128), lambda i: (i // 2, 0, 0, 0, i % 2)),
            pl.BlockSpec((2, 4, 64, 256), lambda i: (0, 0, 0, 0)),
            square, square,
        ],
        out_specs=tuple(
            pl.BlockSpec(b, (lambda i: (0, i)) if n == 1 else (lambda i: (0, 0)))
            for n, (_, _, b) in enumerate(outs)
        ),
        compiler_params=pltpu.CompilerParams(vmem_limit_bytes=16 * 1024 * 1024),
    )(*results, up_accum, down_accum)


def solution(mesh):
    rep_fs, fs = ("rep", "fs"), "fs"
    in_specs = (
        P(rep_fs, "tp"),
        P(rep_fs, "tp"),
        P(rep_fs, None),
        P(rep_fs, "tp"),
        P("tp", fs),
        P(fs, "tp"),
        P(("rep", "tp"), fs),
        P(rep_fs, "tp"),
    )
    out_specs = (
        P(rep_fs, "tp"),
        P(rep_fs, None),
        P(rep_fs, "tp"),
        P(("rep", "tp"), fs),
        P(rep_fs, "tp"),
    )
    return jax.shard_map(local, mesh=mesh, in_specs=in_specs, out_specs=out_specs, check_vma=False)
```

```python
import math

import jax
import jax.numpy as jnp
from jax import lax
from jax.experimental import pallas as pl
from jax.experimental.pallas import tpu as pltpu
from jax.sharding import PartitionSpec as P

BF = jnp.bfloat16
F32 = jnp.float32
MESH = pl.DeviceIdType.MESH

NZ, NY, NX = 8, 4, 4
PARTS = 2
LATER = 0.0
VMEM_MAIN = 60 * 1024 * 1024
W0_READY, W1_READY, EARLY, HOP, LEAD = 35.05, 22.5, 5, 2.5, 0.7
LATE = (40.0, 43.0, 48.0, 52.0, 55.0, 56.0, 61.0)
VMEM_MAIN = 60 * 1024 * 1024
W0_READY, W1_READY, EARLY = 35.05, 19.5, 5
LATE = (40.0, 43.0, 48.0, 52.0, 55.0, 56.0, 61.0)
N_RECV, N_SEND = 142, 19


def dot(a, b, ca, cb):
    return lax.dot_general(a, b, (((ca,), (cb,)), ((), ())), preferred_element_type=F32)


def relu(v):
    return jnp.maximum(v, 0.0)


class Copies:
    def __init__(self, send, recv):
        self.send, self.recv, self.count, self.groups, self.group = send, recv, 0, [], 0

    def slots(self, n):
        self.count += n
        assert self.count <= N_RECV
        return self.count - n

    def begin(self):
        self.groups.append(0)
        self.group = len(self.groups) - 1
        return self.group

    def at(self, slot, group, src, dst, to):
        return pltpu.make_async_remote_copy(
            src_ref=src,
            dst_ref=dst,
            send_sem=self.send.at[group],
            recv_sem=self.recv.at[slot],
            device_id=to,
            device_id_type=MESH,
        )

    def make(self, src, dst, to):
        self.groups[self.group] += math.prod(src.shape)
        return self.at(self.slots(1), self.group, src, dst, to)

    def wait_sent(self, group, size, ref):
        part = ref.at[:, 0:size // 128]
        pltpu.make_async_copy(part, part, self.send.at[group]).wait()


class RingGather:
    def __init__(self, copies, me, block, halves, to):
        up, down = lax.rem(me + 1, 4), lax.rem(me + 3, 4)
        self.to_up = copies.make(block(me), block(me), to(up))
        self.to_down = copies.make(block(me), block(me), to(down))
        self.on_up = copies.make(halves(down)[0], halves(down)[0], to(up))
        self.on_down = copies.make(halves(up)[1], halves(up)[1], to(down))

    def start(self):
        self.to_up.start()
        self.to_down.start()

    def middle(self):
        self.to_up.wait_recv()
        self.on_up.start()
        self.to_down.wait_recv()
        self.on_down.start()

    def end(self):
        self.on_up.wait_recv()
        self.on_down.wait_recv()


class RingReduce:
    def __init__(self, copies, me, block, halves, to, bufs):
        up, down, far = lax.rem(me + 1, 4), lax.rem(me + 3, 4), lax.rem(me + 2, 4)
        self.half_up, self.half_down, self.full_up, self.full_down = bufs
        self.far_up = copies.make(halves(far)[0], self.half_up, to(up))
        self.far_down = copies.make(halves(far)[1], self.half_down, to(down))
        self.near_up = copies.make(block(up), self.full_up, to(up))
        self.near_down = copies.make(block(down), self.full_down, to(down))
        self.sum_up, self.sum_down, self.mine = halves(up)[0], halves(down)[1], block(me)

    def start(self):
        self.far_up.start()
        self.far_down.start()

    def middle(self):
        self.far_up.wait_recv()
        add_into(self.sum_up, self.half_up)
        self.far_down.wait_recv()
        add_into(self.sum_down, self.half_down)
        self.near_up.start()
        self.near_down.start()

    def end(self):
        self.near_up.wait_recv()
        self.near_down.wait_recv()
        return (
            self.mine[...].astype(F32)
            + self.full_up[...].astype(F32)
            + self.full_down[...].astype(F32)
        )


def add_into(total, term):
    total[...] = (total[...].astype(F32) + term[...].astype(F32)).astype(BF)


def line_order(ready, early):
    orders = [[] for _ in range(NZ)]
    for way in (0, 1):
        free = [W1_READY, 26.0, 26.0, 30.0, 30.0, 30.0, 30.0]
        queue = []
        for turn in range(NZ - 1):
            for part in range(PARTS):
                queue.append((ready[1], 1, turn, part) if turn < early else (ready[0] + 0.01, 1, turn, part))
                queue.append((ready[0], 0, turn, part))
        queue.sort()
        for at, weight, turn, part in queue:
            for hop in range(NZ - 1 - turn):
                plane = hop if way == 0 else NZ - 1 - hop
                dest = NZ - 1 - turn if way == 0 else turn
                begin = max(free[hop], at)
                orders[plane].append((max(at, begin - LEAD) if hop == 0 else at, way, weight, dest, part))
                free[hop] = begin + 2.8 / PARTS
                at = begin + 2.8 / PARTS + HOP
    return [sorted(o) for o in orders]


def kernel(
    xn_hbm, xp_hbm, ct_hbm, hp_hbm, up_hbm, dn_hbm,
    out, ig, hng, fr,
    hp, upw, own, tok, wg, hps, hpf, apt, hpo, hpi, hns, an, hg, hgt, rsb, sa, sb,
    a1u, a1d, a2u, a2d, a3u, a3d, a4u, a4d, b1u, b1d, b2u, b2d, b3u, b3d, b4u, b4d,
    grd, line, fg, sums, load, send, recv,
):
    r, f, t = lax.axis_index("rep"), lax.axis_index("fs"), lax.axis_index("tp")
    z, y, x, c = f // NY, lax.rem(f, NY), t // 2, lax.rem(t, 2)
    big_z = r * NZ + z

    def at_x(i):
        return (r, f, i * 2 + c)

    def at_y(j):
        return (r, z * NY + j, t)

    def at_big_z(k):
        return (k // NZ, lax.rem(k, NZ) * NY + y, t)

    partner = (r, f, x * 2 + 1 - c)
    z_up, z_down = at_big_z(lax.rem(big_z + 1, 2 * NZ)), at_big_z(lax.rem(big_z + 2 * NZ - 1, 2 * NZ))
    xs = [lax.rem(x + k, NX) for k in (1, 3, 2)]
    ys = [lax.rem(y + k, NY) for k in (1, 3, 2)]

    loads = [
        pltpu.make_async_copy(source, target, load.at[k])
        for k, (source, target) in enumerate((
            (up_hbm, upw), (dn_hbm, own.at[1]), (dn_hbm.at[x], wg.at[1, x, z]),
            (ct_hbm, tok.at[0, x, y]), (xn_hbm, tok.at[1, x, y]), (xp_hbm, tok.at[2, x, y]), (hp_hbm, hp),
        ))
    ]
    for made in loads:
        made.start()
    barrier = pltpu.get_barrier_semaphore()
    peers = [partner, z_up, z_down] + [at_x(i) for i in xs] + [at_y(j) for j in ys]
    for peer in peers:
        pl.semaphore_signal(barrier, inc=1, device_id=peer, device_id_type=MESH)

    copies = Copies(send, recv)

    for made in loads[:3]:
        made.wait()
    own[0] = upw[...].astype(F32).T.astype(BF).reshape(4, 64, 256)
    wg[0, x, z] = own[0, x]
    with jax.named_scope("barrier"):
        pl.semaphore_wait(barrier, len(peers))

    steps = []

    def at(time, name, act):
        steps.append((time, len(steps), name, act))

    copies.begin()
    spread = {off: copies.make(own.at[:, i], wg.at[:, x, z], at_x(i)) for off, i in ((1, xs[0]), (3, xs[1]), (2, xs[2]))}
    spread[1].start()
    spread[3].start()
    at(4.65, "spread2", lambda: spread[2].start())
    slabs = (x, xs[0], xs[1], xs[2])
    gather_z = {}
    z_group = copies.begin()
    far_groups = (copies.begin(), copies.begin())
    for way, to in ((0, z_up), (1, z_down)):
        for s in range(4):
            piece = lax.rem(z + (NZ - s if way == 0 else s), NZ)
            for k, i in enumerate(slabs):
                place = wg.at[:, i, piece]
                gather_z[way, s, k] = copies.at(
                    copies.slots(1), z_group if s < 3 else far_groups[way], place, place, to
                )

    sends_far = (jnp.logical_and(z >= 3, z <= 6), jnp.logical_and(z >= 1, z <= 4))
    takes_far = (z >= 4, z < 4)

    def begin_z(way, k):
        gather_z[way, 0, k].start()

    def step_z(s, k, way):
        if s <= 3:
            gather_z[way, s - 1, k].wait_recv()
            if s < 3:
                gather_z[way, s, k].start()
            else:
                pl.when(sends_far[way])(lambda: gather_z[way, 3, k].start())
        else:
            pl.when(takes_far[way])(lambda: gather_z[way, 3, k].wait_recv())

    def first_z(k):
        if k:
            spread[(0, 3, 1, 2)[k]].wait_recv()
        begin_z(0, k)
        begin_z(1, k)

    def behind(s):
        return jnp.logical_and(big_z >= 1, big_z <= s)

    def prompt_z(s, k):
        if s <= 3:
            pl.when(jnp.logical_not(behind(s)))(lambda: step_z(s, k, 0))
        else:
            step_z(s, k, 0)
        step_z(s, k, 1)

    def later_z(s, k):
        pl.when(behind(s))(lambda: step_z(s, k, 0))

    z_times = (
        (3.2, 6.5, 6.6, 9.9), (7.15, 10.5, 11.1, 13.3), (13.7, 15.1, 16.5, 18.0),
        (19.5, 21.1, 22.5, 24.1), (25.1, 26.5, 28.0, 29.5),
    )
    for s, row in enumerate(z_times):
        for k, time in enumerate(row):
            if s == 0:
                at(time, f"z{s}{k}", lambda k=k: first_z(k))
            else:
                at(time, f"z{s}{k}", lambda s=s, k=k: prompt_z(s, k))
            if 1 <= s <= 3:
                at(min(time + LATER, 29.8), f"y{s}{k}", lambda s=s, k=k: later_z(s, k))
    for made in loads[3:6]:
        made.wait()
    token_times = {
        (0, 1): ((4.6, 7.25, 10.35), (10.4, 14.95, 18.2), (3.25, 5.8, 8.0), (8.5, 13.2, 16.4)),
        (1, 3): ((11.3, 13.9, 16.75), (16.8, 21.4, 24.6), (3.9, 6.45, 8.7), (15.0, 19.6, 22.8)),
    }
    for (k, end), times in token_times.items():
        copies.begin()
        ks = slice(k, end)
        first = (
            RingGather(
                copies, x,
                lambda i, ks=ks: tok.at[ks, i, y, 0:64],
                lambda i, ks=ks: (tok.at[ks, i, y, 0:32], tok.at[ks, i, y, 32:64]),
                at_x,
            ),
            RingGather(
                copies, y,
                lambda j, ks=ks: tok.at[ks, x, j, 64:128],
                lambda j, ks=ks: (tok.at[ks, x, j, 64:96], tok.at[ks, x, j, 96:128]),
                at_y,
            ),
        )
        second = (
            RingGather(
                copies, y,
                lambda j, ks=ks: tok.at[ks, :, j, 0:64],
                lambda j, ks=ks: (tok.at[ks, 0:2, j, 0:64], tok.at[ks, 2:4, j, 0:64]),
                at_y,
            ),
            RingGather(
                copies, x,
                lambda i, ks=ks: tok.at[ks, i, :, 64:128],
                lambda i, ks=ks: (tok.at[ks, i, 0:2, 64:128], tok.at[ks, i, 2:4, 64:128]),
                at_x,
            ),
        )

        for ring, moments, label in zip((first[0], second[0], first[1], second[1]), times, "abcd"):
            for moment, name in zip(moments, ("start", "middle", "end")):
                at(moment, f"t{k}{label}{name}", getattr(ring, name))

    copies.begin()
    hp_sends = [copies.make(hps.at[j], hpf.at[c, y], at_y(j)) for j in ys]
    hp_pair = copies.make(hpf.at[c], hpf.at[c], partner)

    def hp_first():
        loads[6].wait()
        low = lax.broadcasted_iota(jnp.int32, (128, 128), 1) < 64
        odd = lax.rem(x, 2) == 1
        for j in range(NY):
            for m in range(2):
                off = 1024 * (4 * c + 2 * m) + 256 * j + 128 * (x // 2)
                one = hp[:, pl.ds(pl.multiple_of(off, 128), 128)].astype(F32)
                two = hp[:, pl.ds(pl.multiple_of(off + 1024, 128), 128)].astype(F32)
                left = jnp.where(odd, pltpu.roll(one, 64, axis=1), one)
                right = jnp.where(odd, two, pltpu.roll(two, 64, axis=1))
                hps[j, :, 128 * m:128 * m + 128] = jnp.where(low, left, right).astype(BF)
        hpf[c, y] = hps[y]

    def start_all(made):
        return lambda: [m.start() for m in made]

    def hp_second():
        for m in hp_sends:
            m.wait_recv()
        hp_pair.start()

    def transpose_acts():
        hp_pair.wait_recv()
        for h in range(2):
            for j in range(NY):
                v = relu(hpf[h, j].astype(F32))
                apt[256 * h:256 * h + 256, 128 * j:128 * j + 128] = (v * v).astype(BF).astype(F32).T.astype(BF)

    at(3.4, "hp_first", hp_first)
    at(7.5, "hp_send", start_all(hp_sends))
    at(13.0, "hp_second", hp_second)
    at(14.7, "acts_prev", transpose_acts)

    def partial_gradient(w, left, k):
        def body(i, carry):
            right = tok[k, i].reshape(512, 256)
            for h in range(2):
                got = dot(left[256 * h:256 * h + 256, :], right, 1, 0).astype(BF)
                grd[w, i, 4 * h:4 * h + 4] = got.reshape(4, 64, 256)
            return carry

        lax.fori_loop(0, NX, body, 0)

    at(18.25, "grad1", lambda: partial_gradient(1, apt, 0))

    line_base = copies.slots(2 * PARTS * (NZ + 1))
    line_groups = [copies.begin() for _ in range(NZ)]
    size = NX // PARTS

    def line_copy(way, w, dest, part):
        slot = line_base + (w * PARTS + part) * (NZ + 1) + dest + 1 - way
        place = line.at[way, w, dest, pl.ds(part * size, size)]
        return copies.at(slot, line_groups[0] + dest, place, place, (r, f + NY - 2 * NY * way, t))

    def line_item(way, turn):
        dests = jnp.where(way == 0, NZ - 1 - z, z)
        early = PARTS * jnp.minimum(EARLY, dests)
        late = turn - early - PARTS * dests
        w = jnp.where(jnp.logical_or(turn < early, late >= 0), 1, 0)
        count = jnp.where(turn < early, turn, jnp.where(late < 0, turn - early, early + late))
        nth = count // PARTS
        return w, jnp.where(way == 0, NZ - 1 - nth, nth), lax.rem(count, PARTS)

    orders = line_order((W0_READY, W1_READY), EARLY)
    of_plane = [
        sum((step[1] << n) for n, step in enumerate(order)) for order in orders
    ]

    def for_plane(values):
        found = values[NZ - 1]
        for plane in range(NZ - 1):
            found = jnp.where(z == plane, values[plane], found)
        return found

    ways = [for_plane([bits >> low & (1 << 28) - 1 for bits in of_plane]) for low in (0, 28)]

    def line_body(n, rights):
        way = lax.rem(jnp.where(n < 28, ways[0] >> jnp.minimum(n, 27), ways[1] >> jnp.maximum(n - 28, 0)), 2)
        w, dest, part = line_item(way, jnp.where(way == 0, rights, n - rights))
        made = line_copy(way, w, dest, part)
        inner = jnp.where(way == 0, z > 0, z < NZ - 1)

        @pl.when(inner)
        def _():
            with jax.named_scope("lw"):
                made.wait_recv()

        for i in range(size):
            place = line.at[way, w, dest, part * size + i]
            came = jnp.where(inner, place[...].astype(F32), 0.0)
            place[...] = (came + grd[w, part * size + i, dest].astype(F32)).astype(BF)
        made.start()
        return rights + 1 - way

    line_done = [0, jnp.int32(0), [0] * NZ]

    def line_until(time):
        ends = [sum(step[0] <= time for step in order) for order in orders]
        if ends == line_done[2]:
            return
        end = for_plane(ends)
        line_done[1] = lax.fori_loop(line_done[0], end, line_body, line_done[1])
        line_done[0], line_done[2] = end, ends

    def partial_hidden(q, w):
        def body(j, carry):
            for h in range(2):
                total = None
                for i in range(NX):
                    part = dot(
                        tok[1 - q, i, pl.ds(2 * j, 2)].reshape(256, 256),
                        wg[w, i, 4 * h:4 * h + 4].reshape(256, 256),
                        1, 1,
                    )
                    total = part if total is None else total + part
                hpo[q, h, pl.ds(2 * j, 2)] = total.astype(BF).reshape(2, 128, 256)
            return carry

        lax.fori_loop(0, 2, body, 0)

    copies.begin()
    pair = [copies.make(hpo.at[q], hpi.at[q], partner) for q in range(2)]

    def hidden_sums():
        partial_hidden(1, 1)
        pair[1].start()
        partial_hidden(0, 0)
        pair[0].start()

    def hidden_gradient():
        pair[1].wait_recv()
        for h in range(2):
            for j in range(NY):
                back = hpo[1, h, j].astype(F32) + hpi[1, h, j].astype(F32)
                grad = (back * 2.0 * relu(hpf[h, j].astype(F32))).astype(BF)
                hg[h, j] = grad
                hgt[256 * h:256 * h + 256, 128 * j:128 * j + 128] = grad.astype(F32).T.astype(BF)

    def hidden_acts():
        pair[0].wait_recv()
        for h in range(2):
            for j in range(NY):
                hidden = (hpo[0, h, j].astype(F32) + hpi[0, h, j].astype(F32)).astype(BF)
                hns[h, j] = hidden
                v = relu(hidden.astype(F32))
                an[h, j] = (v * v).astype(BF)

    copies.begin()
    hn_sends = [copies.make(hns.at[c, j], hng.at[c, x, y], at_y(j)) for j in ys]
    hn_ring = RingGather(
        copies, x, lambda i: hng.at[c, i], lambda i: (hng.at[c, i, 0:2], hng.at[c, i, 2:4]), at_x
    )
    hn_pair = [copies.make(hng.at[c, i], hng.at[c, i], partner) for i in [x] + xs]

    hn_own = pltpu.make_async_copy(hns.at[c, y], hng.at[c, x, y], load.at[7])

    def hn_first():
        for m in hn_sends:
            m.start()
        hn_own.start()

    def hn_second():
        hn_own.wait()
        for m in hn_sends:
            m.wait_recv()
        hn_ring.start()
        hn_pair[0].start()

    def hn_third():
        hn_ring.middle()
        hn_pair[1].start()
        hn_pair[2].start()

    def hn_fourth():
        hn_ring.end()
        hn_pair[3].start()

    def partial_output(q, left, w):
        def body(i, carry):
            for j in range(2):
                total = None
                for h in range(2):
                    part = dot(
                        left[h, 2 * j:2 * j + 2].reshape(256, 256),
                        wg[w, i, 4 * h:4 * h + 4].reshape(256, 256),
                        1, 0,
                    )
                    total = part if total is None else total + part
                rsb[q, i, 2 * j:2 * j + 2] = total.astype(BF).reshape(2, 128, 256)
            return carry

        lax.fori_loop(0, NX, body, 0)

    copies.begin()
    reduce_a1 = RingReduce(
        copies, x,
        lambda i: rsb.at[:, i, :, 0:64],
        lambda i: (rsb.at[:, i, 0:2, 0:64], rsb.at[:, i, 2:4, 0:64]),
        at_x, (a1u, a1d, a2u, a2d),
    )
    reduce_b1 = RingReduce(
        copies, y,
        lambda j: rsb.at[:, :, j, 64:128],
        lambda j: (rsb.at[:, 0:2, j, 64:128], rsb.at[:, 2:4, j, 64:128]),
        at_y, (b1u, b1d, b2u, b2d),
    )
    reduce_a2 = RingReduce(
        copies, y,
        lambda j: sa.at[:, j],
        lambda j: (sa.at[:, j, 0:32], sa.at[:, j, 32:64]),
        at_y, (a3u, a3d, a4u, a4d),
    )
    reduce_b2 = RingReduce(
        copies, x,
        lambda i: sb.at[:, i],
        lambda i: (sb.at[:, i, 0:32], sb.at[:, i, 32:64]),
        at_x, (b3u, b3d, b4u, b4d),
    )
    def outputs():
        partial_output(0, an, 1)
        partial_output(1, hg, 0)
        reduce_a1.start()
        reduce_b1.start()

    def reduce_second():
        reduce_a1.middle()
        reduce_b1.middle()

    def reduce_third():
        sa[...] = reduce_a1.end().astype(BF)
        reduce_a2.start()
        sb[...] = reduce_b1.end().astype(BF)
        reduce_b2.start()

    def reduce_fourth():
        reduce_a2.middle()
        reduce_b2.middle()

    results = [
        pltpu.make_async_copy(sums.at[k], ref, load.at[8 + k]) for k, ref in enumerate((out, ig))
    ]

    def reduce_last():
        for rows, ring in ((slice(0, 64), reduce_a2), (slice(64, 128), reduce_b2)):
            total = ring.end()
            sums[0, rows, :] = total[0].astype(BF)
            sums[1, rows, :] = total[1].astype(BF)
        for made in results:
            made.start()

    at(29.9, "hidden", hidden_sums)
    at(32.0, "hidden_grad", hidden_gradient)
    at(33.4, "hidden_acts", hidden_acts)
    at(33.6, "hn1", hn_first)
    at(33.8, "grad0", lambda: partial_gradient(0, hgt, 2))
    at(35.1, "outputs", outputs)
    for time, name, act in zip(
        LATE, ("hn2", "rs2", "hn3", "rs3", "hn4", "rs4", "rs5"),
        (hn_second, reduce_second, hn_third, reduce_third, hn_fourth, reduce_fourth, reduce_last),
    ):
        at(time, name, act)

    for time, _, name, act in sorted(steps, key=lambda step: step[:2]):
        with jax.named_scope(f"line_{name}"):
            line_until(time)
        with jax.named_scope(name):
            act()
    with jax.named_scope("line_rest"):
        line_until(1e9)

    def line_end(w):
        for way, inner in ((0, z > 0), (1, z < NZ - 1)):

            @pl.when(inner)
            def _():
                for part in range(PARTS):
                    line_copy(way, w, z, part).wait_recv()

        fg[w] = (
            grd[w, :, z].astype(F32)
            + jnp.where(z > 0, line[0, w, z].astype(F32), 0.0)
            + jnp.where(z < NZ - 1, line[1, w, z].astype(F32), 0.0)
        ).astype(BF)

    copies.begin()
    final = []
    for w in (1, 0):
        with jax.named_scope("line_end"):
            line_end(w)
        made = [copies.make(fg.at[w, i], fr.at[w, x], at_x(i)) for i in xs]
        kept = pltpu.make_async_copy(fg.at[w, x], fr.at[w, x], load.at[10 + w])
        for m in made + [kept]:
            m.start()
        final += made
        results.append(kept)
    with jax.named_scope("final_wait"):
        for s in hn_pair + final:
            s.wait_recv()
        for s in results:
            s.wait()

    with jax.named_scope("sent"):
        for group, total in enumerate(copies.groups):
            if total:
                copies.wait_sent(group, total, hp)
        copies.wait_sent(z_group, 3 * 2 * 4 * 2 * 64 * 256, hp)
        for way in (0, 1):
            pl.when(sends_far[way])(lambda: copies.wait_sent(far_groups[way], 4 * 2 * 64 * 256, hp))

        def line_sent(dest, carry):
            pl.when(dest != z)(lambda: copies.wait_sent(line_groups[0] + dest, 2 * NX * 64 * 256, hp))
            return carry

        lax.fori_loop(0, NZ, line_sent, 0)
    assert len(copies.groups) <= N_SEND


def finish(raw_out, raw_ig, hng, fr, upa, dna, out, hn_out, ig, ua, da):
    step = pl.program_id(0)
    lanes = pl.ds(pl.multiple_of(lax.rem(step, 2) * 128, 128), 128)

    @pl.when(step == 0)
    def _():
        out[...] = raw_out[...]
        ig[...] = raw_ig[...]
        ua[...] = upa[...] + fr[0].reshape(256, 256).astype(F32).T
        da[...] = dna[...] + fr[1].reshape(256, 256).astype(F32)

    low = lax.broadcasted_iota(jnp.int32, (128, 128), 1) < 64
    for m in range(2):
        for j in range(NY):
            one = hng[step // 2, 2 * m, j, :, lanes].astype(F32)
            two = hng[step // 2, 2 * m + 1, j, :, lanes].astype(F32)
            off = 256 * j + 128 * m
            hn_out[:, off:off + 128] = jnp.where(low, one, pltpu.roll(two, 64, axis=1)).astype(BF)
            hn_out[:, off + 1024:off + 1152] = jnp.where(low, pltpu.roll(one, 64, axis=1), two).astype(BF)


def local(inputs_next, inputs_prev, hidden_prev, cotangent, up_weight, down_weight, up_accum, down_accum):
    vmem = pl.BlockSpec(memory_space=pltpu.VMEM)
    shapes = [
        (128, 8192),
        (256, 256),
        (2, 4, 64, 256),
        (3, 4, 4, 128, 256),
        (2, 4, 8, 64, 256),
        (4, 128, 256),
        (2, 4, 128, 256),
        (512, 512),
        (2, 2, 4, 128, 256),
        (2, 2, 4, 128, 256),
        (2, 4, 128, 256),
        (2, 4, 128, 256),
        (2, 4, 128, 256),
        (512, 512),
        (2, 4, 4, 128, 256),
        (2, 4, 64, 256),
        (2, 4, 64, 256),
    ]
    for _ in range(2):
        shapes += [(2, 2, 64, 256)] * 2 + [(2, 4, 64, 256)] * 2
        shapes += [(2, 32, 256)] * 2 + [(2, 64, 256)] * 2
    shapes += [
        (2, 4, 8, 64, 256),
        (2, 2, 8, 4, 64, 256),
        (2, 4, 64, 256),
        (2, 128, 256),
    ]
    raw = [(128, 256), (128, 256), (2, 4, 4, 128, 256), (2, 4, 64, 256)]
    results = pl.pallas_call(
        kernel,
        out_shape=tuple(pltpu.VMEM(s, BF) for s in raw),
        in_specs=[pl.BlockSpec(memory_space=pltpu.HBM)] * 6,
        out_specs=(pl.BlockSpec(memory_space=pl.ANY),) * 4,
        scratch_shapes=[pltpu.VMEM(s, BF) for s in shapes]
        + [pltpu.SemaphoreType.DMA((12,)), pltpu.SemaphoreType.DMA((N_SEND,)), pltpu.SemaphoreType.DMA((N_RECV,))],
        compiler_params=pltpu.CompilerParams(
            collective_id=0, has_side_effects=True, vmem_limit_bytes=VMEM_MAIN
        ),
    )(inputs_next, inputs_prev, cotangent, hidden_prev, up_weight, down_weight.reshape(4, 64, 256))

    outs = [
        (inputs_next.shape, BF, (128, 256)),
        (hidden_prev.shape, BF, (128, 2048)),
        (inputs_prev.shape, BF, (128, 256)),
        (up_accum.shape, F32, (256, 256)),
        (down_accum.shape, F32, (256, 256)),
    ]
    square = pl.BlockSpec((256, 256), lambda i: (0, 0))
    return pl.pallas_call(
        finish,
        grid=(4,),
        out_shape=tuple(jax.ShapeDtypeStruct(s, d) for s, d, _ in outs),
        in_specs=[
            vmem, vmem, vmem, vmem, square, square,
        ],
        out_specs=tuple(
            pl.BlockSpec(b, (lambda i: (0, i)) if n == 1 else (lambda i: (0, 0)))
            for n, (_, _, b) in enumerate(outs)
        ),
        compiler_params=pltpu.CompilerParams(vmem_limit_bytes=16 * 1024 * 1024),
    )(*results, up_accum, down_accum)


def solution(mesh):
    rep_fs, fs = ("rep", "fs"), "fs"
    in_specs = (
        P(rep_fs, "tp"),
        P(rep_fs, "tp"),
        P(rep_fs, None),
        P(rep_fs, "tp"),
        P("tp", fs),
        P(fs, "tp"),
        P(("rep", "tp"), fs),
        P(rep_fs, "tp"),
    )
    out_specs = (
        P(rep_fs, "tp"),
        P(rep_fs, None),
        P(rep_fs, "tp"),
        P(("rep", "tp"), fs),
        P(rep_fs, "tp"),
    )
    return jax.shard_map(local, mesh=mesh, in_specs=in_specs, out_specs=out_specs, check_vma=False)
```

```python
import math

import jax
import jax.numpy as jnp
from jax import lax
from jax.experimental import pallas as pl
from jax.experimental.pallas import tpu as pltpu
from jax.sharding import PartitionSpec as P

BF = jnp.bfloat16
F32 = jnp.float32
MESH = pl.DeviceIdType.MESH

NZ, NY, NX = 8, 4, 4
PARTS = 2
LATER = 0.0
VMEM_MAIN = 60 * 1024 * 1024
W0_READY, W1_READY, EARLY, HOP, LEAD = 35.05, 22.5, 5, 2.5, 0.7
LATE = (40.0, 43.0, 48.0, 52.0, 55.0, 56.0, 61.0)
VMEM_MAIN = 60 * 1024 * 1024
W0_READY, W1_READY, EARLY = 35.05, 19.5, 5
LATE = (40.0, 43.0, 48.0, 52.0, 55.0, 56.0, 61.0)
N_RECV, N_SEND = 142, 19


def dot(a, b, ca, cb):
    return lax.dot_general(a, b, (((ca,), (cb,)), ((), ())), preferred_element_type=F32)


def relu(v):
    return jnp.maximum(v, 0.0)


class Copies:
    def __init__(self, send, recv):
        self.send, self.recv, self.count, self.groups, self.group = send, recv, 0, [], 0

    def slots(self, n):
        self.count += n
        assert self.count <= N_RECV
        return self.count - n

    def begin(self):
        self.groups.append(0)
        self.group = len(self.groups) - 1
        return self.group

    def at(self, slot, group, src, dst, to):
        return pltpu.make_async_remote_copy(
            src_ref=src,
            dst_ref=dst,
            send_sem=self.send.at[group],
            recv_sem=self.recv.at[slot],
            device_id=to,
            device_id_type=MESH,
        )

    def make(self, src, dst, to):
        self.groups[self.group] += math.prod(src.shape)
        return self.at(self.slots(1), self.group, src, dst, to)

    def wait_sent(self, group, size, ref):
        part = ref.at[:, 0:size // 128]
        pltpu.make_async_copy(part, part, self.send.at[group]).wait()


class RingGather:
    def __init__(self, copies, me, block, halves, to):
        up, down = lax.rem(me + 1, 4), lax.rem(me + 3, 4)
        self.to_up = copies.make(block(me), block(me), to(up))
        self.to_down = copies.make(block(me), block(me), to(down))
        self.on_up = copies.make(halves(down)[0], halves(down)[0], to(up))
        self.on_down = copies.make(halves(up)[1], halves(up)[1], to(down))

    def start(self):
        self.to_up.start()
        self.to_down.start()

    def middle(self):
        self.to_up.wait_recv()
        self.on_up.start()
        self.to_down.wait_recv()
        self.on_down.start()

    def end(self):
        self.on_up.wait_recv()
        self.on_down.wait_recv()


class RingReduce:
    def __init__(self, copies, me, block, halves, to, bufs):
        up, down, far = lax.rem(me + 1, 4), lax.rem(me + 3, 4), lax.rem(me + 2, 4)
        self.half_up, self.half_down, self.full_up, self.full_down = bufs
        self.far_up = copies.make(halves(far)[0], self.half_up, to(up))
        self.far_down = copies.make(halves(far)[1], self.half_down, to(down))
        self.near_up = copies.make(block(up), self.full_up, to(up))
        self.near_down = copies.make(block(down), self.full_down, to(down))
        self.sum_up, self.sum_down, self.mine = halves(up)[0], halves(down)[1], block(me)

    def start(self):
        self.far_up.start()
        self.far_down.start()

    def middle(self):
        self.far_up.wait_recv()
        add_into(self.sum_up, self.half_up)
        self.far_down.wait_recv()
        add_into(self.sum_down, self.half_down)
        self.near_up.start()
        self.near_down.start()

    def end(self):
        self.near_up.wait_recv()
        self.near_down.wait_recv()
        return (
            self.mine[...].astype(F32)
            + self.full_up[...].astype(F32)
            + self.full_down[...].astype(F32)
        )


def add_into(total, term):
    total[...] = (total[...].astype(F32) + term[...].astype(F32)).astype(BF)


def line_order(ready, early):
    orders = [[] for _ in range(NZ)]
    for way in (0, 1):
        free = [W1_READY, 26.0, 26.0, 30.0, 30.0, 30.0, 30.0]
        queue = []
        for turn in range(NZ - 1):
            for part in range(PARTS):
                queue.append((ready[1], 1, turn, part) if turn < early else (ready[0] + 0.01, 1, turn, part))
                queue.append((ready[0], 0, turn, part))
        queue.sort()
        for at, weight, turn, part in queue:
            for hop in range(NZ - 1 - turn):
                plane = hop if way == 0 else NZ - 1 - hop
                dest = NZ - 1 - turn if way == 0 else turn
                begin = max(free[hop], at)
                orders[plane].append((max(at, begin - LEAD) if hop == 0 else at, way, weight, dest, part))
                free[hop] = begin + 2.8 / PARTS
                at = begin + 2.8 / PARTS + HOP
    return [sorted(o) for o in orders]


def kernel(
    xn_hbm, xp_hbm, ct_hbm, hp_hbm, up_hbm, dn_hbm,
    out, ig, hng, fr,
    hp, upw, own, tok, wg, hps, hpf, apt, hpo, hpi, hns, an, hg, hgt, rsb, sa, sb,
    a1u, a1d, a2u, a2d, a3u, a3d, a4u, a4d, b1u, b1d, b2u, b2d, b3u, b3d, b4u, b4d,
    grd, line, fg, sums, load, send, recv,
):
    r, f, t = lax.axis_index("rep"), lax.axis_index("fs"), lax.axis_index("tp")
    z, y, x, c = f // NY, lax.rem(f, NY), t // 2, lax.rem(t, 2)
    big_z = r * NZ + z

    def at_x(i):
        return (r, f, i * 2 + c)

    def at_y(j):
        return (r, z * NY + j, t)

    def at_big_z(k):
        return (k // NZ, lax.rem(k, NZ) * NY + y, t)

    partner = (r, f, x * 2 + 1 - c)
    z_up, z_down = at_big_z(lax.rem(big_z + 1, 2 * NZ)), at_big_z(lax.rem(big_z + 2 * NZ - 1, 2 * NZ))
    xs = [lax.rem(x + k, NX) for k in (1, 3, 2)]
    ys = [lax.rem(y + k, NY) for k in (1, 3, 2)]

    loads = [
        pltpu.make_async_copy(source, target, load.at[k])
        for k, (source, target) in enumerate((
            (up_hbm, upw), (dn_hbm, own.at[1]), (dn_hbm.at[x], wg.at[1, x, z]),
            (ct_hbm, tok.at[0, x, y]), (xn_hbm, tok.at[1, x, y]), (xp_hbm, tok.at[2, x, y]), (hp_hbm, hp),
        ))
    ]
    for made in loads:
        made.start()
    barrier = pltpu.get_barrier_semaphore()
    peers = [partner, z_up, z_down] + [at_x(i) for i in xs] + [at_y(j) for j in ys]
    for peer in peers:
        pl.semaphore_signal(barrier, inc=1, device_id=peer, device_id_type=MESH)

    copies = Copies(send, recv)

    for made in loads[:3]:
        made.wait()
    own[0] = upw[...].astype(F32).T.astype(BF).reshape(4, 64, 256)
    wg[0, x, z] = own[0, x]
    with jax.named_scope("barrier"):
        pl.semaphore_wait(barrier, len(peers))

    steps = []

    def at(time, name, act):
        steps.append((time, len(steps), name, act))

    copies.begin()
    spread = {off: copies.make(own.at[:, i], wg.at[:, x, z], at_x(i)) for off, i in ((1, xs[0]), (3, xs[1]), (2, xs[2]))}
    spread[1].start()
    spread[3].start()
    at(4.65, "spread2", lambda: spread[2].start())
    slabs = (x, xs[0], xs[1], xs[2])
    gather_z = {}
    z_group = copies.begin()
    far_groups = (copies.begin(), copies.begin())
    for way, to in ((0, z_up), (1, z_down)):
        for s in range(4):
            piece = lax.rem(z + (NZ - s if way == 0 else s), NZ)
            for k, i in enumerate(slabs):
                place = wg.at[:, i, piece]
                gather_z[way, s, k] = copies.at(
                    copies.slots(1), z_group if s < 3 else far_groups[way], place, place, to
                )

    sends_far = (jnp.logical_and(z >= 3, z <= 6), jnp.logical_and(z >= 1, z <= 4))
    takes_far = (z >= 4, z < 4)

    def begin_z(way, k):
        gather_z[way, 0, k].start()

    def step_z(s, k, way):
        if s <= 3:
            gather_z[way, s - 1, k].wait_recv()
            if s < 3:
                gather_z[way, s, k].start()
            else:
                pl.when(sends_far[way])(lambda: gather_z[way, 3, k].start())
        else:
            pl.when(takes_far[way])(lambda: gather_z[way, 3, k].wait_recv())

    def first_z(k):
        if k:
            spread[(0, 3, 1, 2)[k]].wait_recv()
        begin_z(0, k)
        begin_z(1, k)

    def behind(s):
        return jnp.logical_and(big_z >= 1, big_z <= s)

    def prompt_z(s, k):
        if s <= 3:
            pl.when(jnp.logical_not(behind(s)))(lambda: step_z(s, k, 0))
        else:
            step_z(s, k, 0)
        step_z(s, k, 1)

    def later_z(s, k):
        pl.when(behind(s))(lambda: step_z(s, k, 0))

    z_times = (
        (3.2, 6.5, 6.6, 9.9), (7.15, 10.5, 11.1, 13.3), (13.7, 15.1, 16.5, 18.0),
        (19.5, 21.1, 22.5, 24.1), (25.1, 26.5, 28.0, 29.5),
    )
    for s, row in enumerate(z_times):
        for k, time in enumerate(row):
            if s == 0:
                at(time, f"z{s}{k}", lambda k=k: first_z(k))
            else:
                at(time, f"z{s}{k}", lambda s=s, k=k: prompt_z(s, k))
            if 1 <= s <= 3:
                at(min(time + LATER, 29.8), f"y{s}{k}", lambda s=s, k=k: later_z(s, k))
    for made in loads[3:6]:
        made.wait()
    token_times = {
        (0, 1): ((4.6, 7.25, 10.35), (10.4, 14.95, 18.2), (3.25, 5.8, 8.0), (8.5, 13.2, 16.4)),
        (1, 3): ((11.3, 13.9, 16.75), (16.8, 21.4, 24.6), (3.9, 6.45, 8.7), (15.0, 19.6, 22.8)),
    }
    for (k, end), times in token_times.items():
        copies.begin()
        ks = slice(k, end)
        first = (
            RingGather(
                copies, x,
                lambda i, ks=ks: tok.at[ks, i, y, 0:64],
                lambda i, ks=ks: (tok.at[ks, i, y, 0:32], tok.at[ks, i, y, 32:64]),
                at_x,
            ),
            RingGather(
                copies, y,
                lambda j, ks=ks: tok.at[ks, x, j, 64:128],
                lambda j, ks=ks: (tok.at[ks, x, j, 64:96], tok.at[ks, x, j, 96:128]),
                at_y,
            ),
        )
        second = (
            RingGather(
                copies, y,
                lambda j, ks=ks: tok.at[ks, :, j, 0:64],
                lambda j, ks=ks: (tok.at[ks, 0:2, j, 0:64], tok.at[ks, 2:4, j, 0:64]),
                at_y,
            ),
            RingGather(
                copies, x,
                lambda i, ks=ks: tok.at[ks, i, :, 64:128],
                lambda i, ks=ks: (tok.at[ks, i, 0:2, 64:128], tok.at[ks, i, 2:4, 64:128]),
                at_x,
            ),
        )

        for ring, moments, label in zip((first[0], second[0], first[1], second[1]), times, "abcd"):
            for moment, name in zip(moments, ("start", "middle", "end")):
                at(moment, f"t{k}{label}{name}", getattr(ring, name))

    copies.begin()
    hp_sends = [copies.make(hps.at[j], hpf.at[c, y], at_y(j)) for j in ys]
    hp_pair = copies.make(hpf.at[c], hpf.at[c], partner)

    def hp_first():
        loads[6].wait()
        low = lax.broadcasted_iota(jnp.int32, (128, 128), 1) < 64
        odd = lax.rem(x, 2) == 1
        for j in range(NY):
            for m in range(2):
                off = 1024 * (4 * c + 2 * m) + 256 * j + 128 * (x // 2)
                one = hp[:, pl.ds(pl.multiple_of(off, 128), 128)].astype(F32)
                two = hp[:, pl.ds(pl.multiple_of(off + 1024, 128), 128)].astype(F32)
                left = jnp.where(odd, pltpu.roll(one, 64, axis=1), one)
                right = jnp.where(odd, two, pltpu.roll(two, 64, axis=1))
                hps[j, :, 128 * m:128 * m + 128] = jnp.where(low, left, right).astype(BF)
        hpf[c, y] = hps[y]

    def start_all(made):
        return lambda: [m.start() for m in made]

    def hp_second():
        for m in hp_sends:
            m.wait_recv()
        hp_pair.start()

    def transpose_acts():
        hp_pair.wait_recv()
        for h in range(2):
            for j in range(NY):
                v = relu(hpf[h, j].astype(F32))
                apt[256 * h:256 * h + 256, 128 * j:128 * j + 128] = (v * v).astype(BF).astype(F32).T.astype(BF)

    at(3.4, "hp_first", hp_first)
    at(7.5, "hp_send", start_all(hp_sends))
    at(13.0, "hp_second", hp_second)
    at(14.7, "acts_prev", transpose_acts)

    def partial_gradient(w, left, k):
        def body(i, carry):
            right = tok[k, i].reshape(512, 256)
            for h in range(2):
                got = dot(left[256 * h:256 * h + 256, :], right, 1, 0).astype(BF)
                grd[w, i, 4 * h:4 * h + 4] = got.reshape(4, 64, 256)
            return carry

        lax.fori_loop(0, NX, body, 0)

    at(18.25, "grad1", lambda: partial_gradient(1, apt, 0))

    line_base = copies.slots(2 * PARTS * (NZ + 1))
    line_groups = [copies.begin() for _ in range(NZ)]
    size = NX // PARTS

    def line_copy(way, w, dest, part):
        slot = line_base + (w * PARTS + part) * (NZ + 1) + dest + 1 - way
        place = line.at[way, w, dest, pl.ds(part * size, size)]
        return copies.at(slot, line_groups[0] + dest, place, place, (r, f + NY - 2 * NY * way, t))

    def line_item(way, turn):
        dests = jnp.where(way == 0, NZ - 1 - z, z)
        early = PARTS * jnp.minimum(EARLY, dests)
        late = turn - early - PARTS * dests
        w = jnp.where(jnp.logical_or(turn < early, late >= 0), 1, 0)
        count = jnp.where(turn < early, turn, jnp.where(late < 0, turn - early, early + late))
        nth = count // PARTS
        return w, jnp.where(way == 0, NZ - 1 - nth, nth), lax.rem(count, PARTS)

    orders = line_order((W0_READY, W1_READY), EARLY)
    of_plane = [
        sum((step[1] << n) for n, step in enumerate(order)) for order in orders
    ]

    def for_plane(values):
        found = values[NZ - 1]
        for plane in range(NZ - 1):
            found = jnp.where(z == plane, values[plane], found)
        return found

    ways = [for_plane([bits >> low & (1 << 28) - 1 for bits in of_plane]) for low in (0, 28)]

    def line_body(n, rights):
        way = lax.rem(jnp.where(n < 28, ways[0] >> jnp.minimum(n, 27), ways[1] >> jnp.maximum(n - 28, 0)), 2)
        w, dest, part = line_item(way, jnp.where(way == 0, rights, n - rights))
        made = line_copy(way, w, dest, part)
        inner = jnp.where(way == 0, z > 0, z < NZ - 1)

        @pl.when(inner)
        def _():
            with jax.named_scope("lw"):
                made.wait_recv()

        for i in range(size):
            place = line.at[way, w, dest, part * size + i]
            came = jnp.where(inner, place[...].astype(F32), 0.0)
            place[...] = (came + grd[w, part * size + i, dest].astype(F32)).astype(BF)
        made.start()
        return rights + 1 - way

    line_done = [0, jnp.int32(0), [0] * NZ]

    def line_until(time):
        ends = [sum(step[0] <= time for step in order) for order in orders]
        if ends == line_done[2]:
            return
        end = for_plane(ends)
        line_done[1] = lax.fori_loop(line_done[0], end, line_body, line_done[1])
        line_done[0], line_done[2] = end, ends

    def partial_hidden(q, w):
        def body(j, carry):
            for h in range(2):
                total = None
                for i in range(NX):
                    part = dot(
                        tok[1 - q, i, pl.ds(2 * j, 2)].reshape(256, 256),
                        wg[w, i, 4 * h:4 * h + 4].reshape(256, 256),
                        1, 1,
                    )
                    total = part if total is None else total + part
                hpo[q, h, pl.ds(2 * j, 2)] = total.astype(BF).reshape(2, 128, 256)
            return carry

        lax.fori_loop(0, 2, body, 0)

    copies.begin()
    pair = [copies.make(hpo.at[q], hpi.at[q], partner) for q in range(2)]

    def hidden_sums():
        partial_hidden(1, 1)
        pair[1].start()
        partial_hidden(0, 0)
        pair[0].start()

    def hidden_gradient():
        pair[1].wait_recv()
        for h in range(2):
            for j in range(NY):
                back = hpo[1, h, j].astype(F32) + hpi[1, h, j].astype(F32)
                grad = (back * 2.0 * relu(hpf[h, j].astype(F32))).astype(BF)
                hg[h, j] = grad
                hgt[256 * h:256 * h + 256, 128 * j:128 * j + 128] = grad.astype(F32).T.astype(BF)

    def hidden_acts():
        pair[0].wait_recv()
        for h in range(2):
            for j in range(NY):
                hidden = (hpo[0, h, j].astype(F32) + hpi[0, h, j].astype(F32)).astype(BF)
                hns[h, j] = hidden
                v = relu(hidden.astype(F32))
                an[h, j] = (v * v).astype(BF)

    copies.begin()
    hn_sends = [copies.make(hns.at[c, j], hng.at[c, x, y], at_y(j)) for j in ys]
    hn_ring = RingGather(
        copies, x, lambda i: hng.at[c, i], lambda i: (hng.at[c, i, 0:2], hng.at[c, i, 2:4]), at_x
    )
    hn_pair = [copies.make(hng.at[c, i], hng.at[c, i], partner) for i in [x] + xs]

    hn_own = pltpu.make_async_copy(hns.at[c, y], hng.at[c, x, y], load.at[7])

    def hn_first():
        for m in hn_sends:
            m.start()
        hn_own.start()

    def hn_second():
        hn_own.wait()
        for m in hn_sends:
            m.wait_recv()
        hn_ring.start()
        hn_pair[0].start()

    def hn_third():
        hn_ring.middle()
        hn_pair[1].start()
        hn_pair[2].start()

    def hn_fourth():
        hn_ring.end()
        hn_pair[3].start()

    def partial_output(q, left, w):
        def body(i, carry):
            for j in range(2):
                total = None
                for h in range(2):
                    part = dot(
                        left[h, 2 * j:2 * j + 2].reshape(256, 256),
                        wg[w, i, 4 * h:4 * h + 4].reshape(256, 256),
                        1, 0,
                    )
                    total = part if total is None else total + part
                rsb[q, i, 2 * j:2 * j + 2] = total.astype(BF).reshape(2, 128, 256)
            return carry

        lax.fori_loop(0, NX, body, 0)

    copies.begin()
    reduce_a1 = RingReduce(
        copies, x,
        lambda i: rsb.at[:, i, :, 0:64],
        lambda i: (rsb.at[:, i, 0:2, 0:64], rsb.at[:, i, 2:4, 0:64]),
        at_x, (a1u, a1d, a2u, a2d),
    )
    reduce_b1 = RingReduce(
        copies, y,
        lambda j: rsb.at[:, :, j, 64:128],
        lambda j: (rsb.at[:, 0:2, j, 64:128], rsb.at[:, 2:4, j, 64:128]),
        at_y, (b1u, b1d, b2u, b2d),
    )
    reduce_a2 = RingReduce(
        copies, y,
        lambda j: sa.at[:, j],
        lambda j: (sa.at[:, j, 0:32], sa.at[:, j, 32:64]),
        at_y, (a3u, a3d, a4u, a4d),
    )
    reduce_b2 = RingReduce(
        copies, x,
        lambda i: sb.at[:, i],
        lambda i: (sb.at[:, i, 0:32], sb.at[:, i, 32:64]),
        at_x, (b3u, b3d, b4u, b4d),
    )
    def outputs():
        partial_output(0, an, 1)
        partial_output(1, hg, 0)
        reduce_a1.start()
        reduce_b1.start()

    def reduce_second():
        reduce_a1.middle()
        reduce_b1.middle()

    def reduce_third():
        sa[...] = reduce_a1.end().astype(BF)
        reduce_a2.start()
        sb[...] = reduce_b1.end().astype(BF)
        reduce_b2.start()

    def reduce_fourth():
        reduce_a2.middle()
        reduce_b2.middle()

    results = [
        pltpu.make_async_copy(sums.at[k], ref, load.at[8 + k]) for k, ref in enumerate((out, ig))
    ]

    def reduce_last():
        for rows, ring in ((slice(0, 64), reduce_a2), (slice(64, 128), reduce_b2)):
            total = ring.end()
            sums[0, rows, :] = total[0].astype(BF)
            sums[1, rows, :] = total[1].astype(BF)
        for made in results:
            made.start()

    at(29.9, "hidden", hidden_sums)
    at(32.0, "hidden_grad", hidden_gradient)
    at(33.4, "hidden_acts", hidden_acts)
    at(33.6, "hn1", hn_first)
    at(33.8, "grad0", lambda: partial_gradient(0, hgt, 2))
    at(35.1, "outputs", outputs)
    for time, name, act in zip(
        LATE, ("hn2", "rs2", "hn3", "rs3", "hn4", "rs4", "rs5"),
        (hn_second, reduce_second, hn_third, reduce_third, hn_fourth, reduce_fourth, reduce_last),
    ):
        at(time, name, act)

    for time, _, name, act in sorted(steps, key=lambda step: step[:2]):
        with jax.named_scope(f"line_{name}"):
            line_until(time)
        with jax.named_scope(name):
            act()
    with jax.named_scope("line_rest"):
        line_until(1e9)

    def line_end(w):
        for way, inner in ((0, z > 0), (1, z < NZ - 1)):

            @pl.when(inner)
            def _():
                for part in range(PARTS):
                    line_copy(way, w, z, part).wait_recv()

        fg[w] = (
            grd[w, :, z].astype(F32)
            + jnp.where(z > 0, line[0, w, z].astype(F32), 0.0)
            + jnp.where(z < NZ - 1, line[1, w, z].astype(F32), 0.0)
        ).astype(BF)

    copies.begin()
    final = []
    for w in (1, 0):
        with jax.named_scope("line_end"):
            line_end(w)
        made = [copies.make(fg.at[w, i], fr.at[w, x], at_x(i)) for i in xs]
        kept = pltpu.make_async_copy(fg.at[w, x], fr.at[w, x], load.at[10 + w])
        for m in made[::-1] + [kept]:
            m.start()
        final += made
        results.append(kept)
    with jax.named_scope("final_wait"):
        for s in hn_pair + final:
            s.wait_recv()
        for s in results:
            s.wait()

    with jax.named_scope("sent"):
        for group, total in enumerate(copies.groups):
            if total:
                copies.wait_sent(group, total, hp)
        copies.wait_sent(z_group, 3 * 2 * 4 * 2 * 64 * 256, hp)
        for way in (0, 1):
            pl.when(sends_far[way])(lambda: copies.wait_sent(far_groups[way], 4 * 2 * 64 * 256, hp))

        def line_sent(dest, carry):
            pl.when(dest != z)(lambda: copies.wait_sent(line_groups[0] + dest, 2 * NX * 64 * 256, hp))
            return carry

        lax.fori_loop(0, NZ, line_sent, 0)
    assert len(copies.groups) <= N_SEND


def finish(raw_out, raw_ig, hng, fr, upa, dna, out, hn_out, ig, ua, da):
    step = pl.program_id(0)
    lanes = pl.ds(pl.multiple_of(lax.rem(step, 2) * 128, 128), 128)

    @pl.when(step == 0)
    def _():
        out[...] = raw_out[...]
        ig[...] = raw_ig[...]
        ua[...] = upa[...] + fr[0].reshape(256, 256).astype(F32).T
        da[...] = dna[...] + fr[1].reshape(256, 256).astype(F32)

    low = lax.broadcasted_iota(jnp.int32, (128, 128), 1) < 64
    for m in range(2):
        for j in range(NY):
            one = hng[step // 2, 2 * m, j, :, lanes].astype(F32)
            two = hng[step // 2, 2 * m + 1, j, :, lanes].astype(F32)
            off = 256 * j + 128 * m
            hn_out[:, off:off + 128] = jnp.where(low, one, pltpu.roll(two, 64, axis=1)).astype(BF)
            hn_out[:, off + 1024:off + 1152] = jnp.where(low, pltpu.roll(one, 64, axis=1), two).astype(BF)


def local(inputs_next, inputs_prev, hidden_prev, cotangent, up_weight, down_weight, up_accum, down_accum):
    vmem = pl.BlockSpec(memory_space=pltpu.VMEM)
    shapes = [
        (128, 8192),
        (256, 256),
        (2, 4, 64, 256),
        (3, 4, 4, 128, 256),
        (2, 4, 8, 64, 256),
        (4, 128, 256),
        (2, 4, 128, 256),
        (512, 512),
        (2, 2, 4, 128, 256),
        (2, 2, 4, 128, 256),
        (2, 4, 128, 256),
        (2, 4, 128, 256),
        (2, 4, 128, 256),
        (512, 512),
        (2, 4, 4, 128, 256),
        (2, 4, 64, 256),
        (2, 4, 64, 256),
    ]
    for _ in range(2):
        shapes += [(2, 2, 64, 256)] * 2 + [(2, 4, 64, 256)] * 2
        shapes += [(2, 32, 256)] * 2 + [(2, 64, 256)] * 2
    shapes += [
        (2, 4, 8, 64, 256),
        (2, 2, 8, 4, 64, 256),
        (2, 4, 64, 256),
        (2, 128, 256),
    ]
    raw = [(128, 256), (128, 256), (2, 4, 4, 128, 256), (2, 4, 64, 256)]
    results = pl.pallas_call(
        kernel,
        out_shape=tuple(pltpu.VMEM(s, BF) for s in raw),
        in_specs=[pl.BlockSpec(memory_space=pltpu.HBM)] * 6,
        out_specs=(pl.BlockSpec(memory_space=pl.ANY),) * 4,
        scratch_shapes=[pltpu.VMEM(s, BF) for s in shapes]
        + [pltpu.SemaphoreType.DMA((12,)), pltpu.SemaphoreType.DMA((N_SEND,)), pltpu.SemaphoreType.DMA((N_RECV,))],
        compiler_params=pltpu.CompilerParams(
            collective_id=0, has_side_effects=True, vmem_limit_bytes=VMEM_MAIN
        ),
    )(inputs_next, inputs_prev, cotangent, hidden_prev, up_weight, down_weight.reshape(4, 64, 256))

    outs = [
        (inputs_next.shape, BF, (128, 256)),
        (hidden_prev.shape, BF, (128, 2048)),
        (inputs_prev.shape, BF, (128, 256)),
        (up_accum.shape, F32, (256, 256)),
        (down_accum.shape, F32, (256, 256)),
    ]
    square = pl.BlockSpec((256, 256), lambda i: (0, 0))
    return pl.pallas_call(
        finish,
        grid=(4,),
        out_shape=tuple(jax.ShapeDtypeStruct(s, d) for s, d, _ in outs),
        in_specs=[
            vmem, vmem, vmem, vmem, square, square,
        ],
        out_specs=tuple(
            pl.BlockSpec(b, (lambda i: (0, i)) if n == 1 else (lambda i: (0, 0)))
            for n, (_, _, b) in enumerate(outs)
        ),
        compiler_params=pltpu.CompilerParams(vmem_limit_bytes=16 * 1024 * 1024),
    )(*results, up_accum, down_accum)


def solution(mesh):
    rep_fs, fs = ("rep", "fs"), "fs"
    in_specs = (
        P(rep_fs, "tp"),
        P(rep_fs, "tp"),
        P(rep_fs, None),
        P(rep_fs, "tp"),
        P("tp", fs),
        P(fs, "tp"),
        P(("rep", "tp"), fs),
        P(rep_fs, "tp"),
    )
    out_specs = (
        P(rep_fs, "tp"),
        P(rep_fs, None),
        P(rep_fs, "tp"),
        P(("rep", "tp"), fs),
        P(rep_fs, "tp"),
    )
    return jax.shard_map(local, mesh=mesh, in_specs=in_specs, out_specs=out_specs, check_vma=False)
```
